512 devices in a mesh: grp: 2 (over y), fs: 32 (over z), tp: 8 (over x, core).
Axes of the slice: x: 4, y: 2, z: 32, core: 2. Of those that a mesh axis runs over, the one named last changes fastest.
The devices are a block of a 4x8x32 slice.
Arguments:
- tokens: bfloat16 [64, 384, 2048], P(('grp', 'fs'), None, 'tp'), parts along dimension 0, may hold values from -16 to 16
- norm_gain: float32 [2048], P('tp'), may hold values from 0.1 to 1.9
- in_weight: bfloat16 [2048, 1024], P('fs', 'tp'), may hold values from -0.125 to 0.125
- pool_weight: bfloat16 [8, 128, 128], P('tp'), may hold values from -0.5 to 0.5
- pool_scale: float32 [1024], P('tp'), may hold values from 0.1 to 1.9
- out_weight: bfloat16 [1024, 2048], P('fs', 'tp'), may hold values from -0.1875 to 0.1875
- ffn_gain: float32 [2048], P('tp'), may hold values from 0.1 to 1.9
- gate_weight: bfloat16 [2048, 5632], P('fs', 'tp'), may hold values from -0.125 to 0.125
- up_weight: bfloat16 [2048, 5632], P('fs', 'tp'), may hold values from -0.125 to 0.125
- down_weight: bfloat16 [5632, 2048], P('tp', 'fs'), may hold values from -0.078125 to 0.078125
Outputs:
- output: bfloat16 [64, 384, 2048], P(('grp', 'fs'), None, 'tp'), parts along dimension 0
The draws below stay inside these ranges and needn't reach their ends.
There are 2 independent parts, one for each index of `grp`. The reference program is written for one: setup_inputs(seed, part) draws one part's arguments, and reference() takes and returns one part's arrays. A program takes and returns all parts, laid end to end along the dimension named above; an argument that names none is the same for every part. Nothing has to cross between parts.
All inputs are finite; a program needn't handle non-finite values.
Results may differ from the reference program's by a relative error of at most 0.009.
Values may be sent and summed in bfloat16 or wider, within the bound.
No kernel may reach another device: no remote copies, remote signals or barrier semaphores. Data moves between devices by JAX's collectives and lax.ppermute only.
A program may use at most 64 MiB of HBM per device.

```python
import jax
import jax.numpy as jnp
from jax import lax

D = 2048
FF = 5632
GROUPS = 8
GD = 128
PW = 1024
LEN = 384
SEQS = 32
N_TP = 8


def draw_tokens(key, part):
    base_key = jax.random.fold_in(key, 11)
    noise_key, block_key, row_key = jax.random.split(base_key, 3)
    noise_draw = jax.random.normal(noise_key, (SEQS, LEN, D), jnp.float32)
    block_scale = jnp.exp(jax.random.uniform(block_key, (16,), jnp.float32, -1.4, 1.4))
    row_scale = jnp.exp(jax.random.uniform(row_key, (SEQS, LEN, 1), jnp.float32, -0.5, 0.5))
    return jnp.clip(noise_draw * jnp.repeat(block_scale, D // 16) * row_scale, -16.0, 16.0).astype(jnp.bfloat16)


def level_of(stream_key, shape, cuts, least, high):
    level, own = 1.0, jax.random.fold_in(stream_key, 6)
    for axis_at, parts in cuts:
        draws = jnp.exp(jax.random.uniform(jax.random.fold_in(own, axis_at), (parts,), jnp.float32, least / len(cuts), high / len(cuts)))
        level = level * jnp.repeat(draws, shape[axis_at] // parts).reshape([-1 if axis == axis_at else 1 for axis in range(len(shape))])
    return level


def gaussian(key, extent, scale, reach, cuts=(), held_as=jnp.bfloat16):
    entries = scale * jax.random.normal(key, extent, jnp.float32)
    if cuts:
        entries = entries * level_of(key, extent, cuts, -0.22, 0.18)
    return jnp.clip(entries, -reach, reach).astype(held_as)


def setup_inputs(seed: int = 0, part: int = 0) -> dict:
    splits = jax.random.split(jax.random.key(seed), 11)
    part_keys = jax.random.split(jax.random.fold_in(splits[10], part), 11)
    return {
        "tokens": draw_tokens(jax.random.fold_in(jax.random.fold_in(splits[10], part), 71), part),
        "norm_gain": jnp.clip(1.0 + 0.18 * jax.random.normal(splits[1], (D,), jnp.float32), 0.1, 1.9),
        "in_weight": gaussian(splits[2], (D, PW), D ** -0.5, 0.125, ((0, 32), (1, 8))),
        "pool_weight": gaussian(splits[3], (GROUPS, GD, GD), GD ** -0.5, 0.5, ((0, 8),)),
        "pool_scale": jnp.clip(1.0 + 0.18 * jax.random.normal(splits[4], (PW,), jnp.float32), 0.1, 1.9),
        "out_weight": gaussian(splits[5], (PW, D), PW ** -0.5, 0.1875, ((0, 32), (1, 8))),
        "ffn_gain": jnp.clip(1.0 + 0.18 * jax.random.normal(splits[6], (D,), jnp.float32), 0.1, 1.9),
        "gate_weight": gaussian(splits[7], (D, FF), D ** -0.5, 0.125, ((0, 32), (1, 8))),
        "up_weight": gaussian(splits[8], (D, FF), D ** -0.5, 0.125, ((0, 32), (1, 8))),
        "down_weight": gaussian(splits[9], (FF, D), FF ** -0.5, 0.078125, ((0, 8), (1, 32))),
    }


EPSILON = 0.05
HALVES = (1, 2, 4, 8)

def norm_rows(stream, gain):
    square = lax.optimization_barrier(jnp.sum(stream * stream, axis=-1, keepdims=True))
    return (stream * lax.rsqrt(square / stream.shape[-1] + EPSILON) * gain).astype(jnp.bfloat16)

def reference(tokens, norm_gain, in_weight, pool_weight, pool_scale, out_weight, ffn_gain, gate_weight, up_weight, down_weight):
    seq_count, length, width = tokens.shape
    stream = tokens.astype(jnp.float32).reshape(seq_count * length, width)
    normed = norm_rows(stream, norm_gain)
    pool_input = jnp.dot(normed, in_weight, preferred_element_type=jnp.float32).astype(jnp.bfloat16)
    pool_float = pool_input.astype(jnp.float32).reshape(seq_count, length, -1)
    running = jnp.concatenate([jnp.zeros((seq_count, 1, pool_float.shape[2]), jnp.float32), jnp.cumsum(pool_float, axis=1)], axis=1)
    position = jnp.arange(length)
    blocks = []
    for group in range(GROUPS):
        half_width = HALVES[group % 4]
        lower_index = jnp.clip(position - half_width, 0, length)
        upper_index = jnp.clip(position + half_width, 0, length)
        group_sums = running[:, :, group * GD:(group + 1) * GD]
        counts = (upper_index - lower_index).astype(jnp.float32)
        window_mean = (group_sums[:, upper_index] - group_sums[:, lower_index]) / counts[:, None]
        blocks.append(window_mean - pool_float[:, :, group * GD:(group + 1) * GD])
    deviation = jnp.stack(blocks, axis=2).astype(jnp.bfloat16)
    mapped = jnp.einsum('slgc,gcd->slgd', deviation.astype(jnp.float32), pool_weight.astype(jnp.float32))
    pooled = (mapped.reshape(seq_count * length, GROUPS * GD) * pool_scale).astype(jnp.bfloat16)
    mixed = stream + jnp.dot(pooled, out_weight, preferred_element_type=jnp.float32)
    normed_two = norm_rows(mixed, ffn_gain)
    gate_out = jnp.dot(normed_two, gate_weight, preferred_element_type=jnp.float32)
    up_out = jnp.dot(normed_two, up_weight, preferred_element_type=jnp.float32)
    hidden = (jax.nn.silu(gate_out) * up_out).astype(jnp.bfloat16)
    block_size = FF // N_TP
    summed = jnp.zeros_like(mixed)
    for block_index in range(N_TP):
        lower_unit = block_index * block_size
        partial_value = jnp.dot(hidden[:, lower_unit:lower_unit + block_size], down_weight[lower_unit:lower_unit + block_size], preferred_element_type=jnp.float32).astype(jnp.bfloat16)
        summed = summed + partial_value.astype(jnp.float32)
    return (mixed + summed).astype(jnp.bfloat16).reshape(seq_count, length, width)
```

```python
import functools

import jax
import jax.numpy as jnp
from jax import lax
from jax.experimental import pallas as pl
from jax.experimental.pallas import tpu as pltpu
from jax.sharding import Mesh
from jax.sharding import PartitionSpec as P

D = 2048
GD = 128
EPSILON = 0.05
CORES = 2
LANES = 128
EXTRA = 16
VM = pltpu.VMEM
F32, BF16 = jnp.float32, jnp.bfloat16


def dot(a, b):
    return lax.dot_general(a, b, (((1,), (0,)), ((), ())), preferred_element_type=F32)


def dot_t(a, b):
    return lax.dot_general(a, b, (((1,), (1,)), ((), ())), preferred_element_type=F32)


def pieces(gain):
    high = lax.reduce_precision(gain, 8, 7)
    rest = gain - high
    mid = lax.reduce_precision(rest, 8, 7)
    return [high, mid, rest - mid]


def gain_row(block, at):
    rows = block[at : at + 3, :].astype(F32)
    return rows[0:1] + rows[1:2] + rows[2:3]


def spec(where=VM):
    return pl.BlockSpec(memory_space=where)


def mixer_kernel(scal, own, other, weight, pool_weight, pool_scale, pooled):
    core, half_width = scal[0], scal[1]
    chips = own.shape[0]
    length, width = own.shape[1] - EXTRA, own.shape[2]
    square = jnp.zeros((length, 1), F32)
    for side in (own, other):
        for chip in range(chips):
            part = side[chip, :length, :].astype(F32)
            square += jnp.sum(part * part, axis=1, keepdims=True)
    scale = lax.rsqrt(square / D + EPSILON)
    total = jnp.zeros((length, weight.shape[1]), F32)
    for which, side in ((core, own), (1 - core, other)):
        for chip in range(chips):
            gain = gain_row(side[chip, length:, :], 0)
            part = side[chip, :length, :].astype(F32)
            normed = (part * scale * gain).astype(BF16)
            row = pl.multiple_of((chip * CORES + which) * width, width)
            total += dot(normed, weight[pl.ds(row, width), :])
    pool_input = total.astype(BF16)
    row = lax.broadcasted_iota(jnp.int32, (length, length), 0)
    column = lax.broadcasted_iota(jnp.int32, (length, length), 1)
    inside = (column >= row - half_width) & (column < row + half_width)
    window = dot(inside.astype(F32).astype(BF16), pool_input)
    at = lax.broadcasted_iota(jnp.int32, (length, 1), 0)
    count = jnp.minimum(at + half_width, length) - jnp.maximum(at - half_width, 0)
    deviation = (window / count.astype(F32) - pool_input.astype(F32)).astype(BF16)
    mapped = dot(deviation, pool_weight[0])
    pooled[...] = (mapped * pool_scale[...]).astype(BF16)


def out_kernel(pooled, weight, tokens, gain, mixed, scaled):
    total = tokens[...].astype(F32)
    depth = pooled.shape[2]
    add = jnp.zeros_like(total)
    for block in range(pooled.shape[0]):
        add += dot(pooled[block], weight[pl.ds(block * depth, depth), :])
    total = total + add
    mixed[...] = total
    scaled[...] = (total * gain[...]).astype(BF16)


def square_kernel(own, other, own_gain, other_gain, scale):
    length = own.shape[1]
    square = jnp.zeros((length, 1), F32)
    for side, gains in ((own, own_gain), (other, other_gain)):
        for chip in range(own.shape[0]):
            gain = gain_row(gains[chip], 3)
            part = side[chip].astype(F32)
            square += jnp.sum(part * part * (1.0 / (gain * gain)), axis=1, keepdims=True)
    scale[...] = jnp.broadcast_to(lax.rsqrt(square / D + EPSILON), scale.shape)


def hidden_kernel(scal, own, other, scale, weight, hidden, partial, wide, down, sems, dsems):
    core = scal[0]
    chips, length, width = own.shape
    blocks = wide.shape[0]

    def gate_copy(i):
        return pltpu.make_async_copy(
            weight.at[:, pl.ds(i * 2 * LANES, 2 * LANES)], wide.at[i], sems.at[i]
        )

    def down_copy(chip):
        row = pl.multiple_of((chip * CORES + 1 - core) * width, width)
        return pltpu.make_async_copy(
            weight.at[pl.ds(row, width), pl.ds(weight.shape[1] - down.shape[2], down.shape[2])],
            down.at[chip],
            dsems.at[chip],
        )

    for i in range(blocks):
        gate_copy(i).start()
    for chip in range(chips):
        down_copy(chip).start()
    factor = scale[...]

    def product(i, columns):
        total = jnp.zeros((length, columns), F32)
        for which, side in ((core, own), (1 - core, other)):
            for chip in range(chips):
                row = pl.multiple_of((chip * CORES + which) * width, width)
                total += dot(side[chip], wide[i, pl.ds(row, width), :columns])
        return total

    def activated(gate, up):
        return (gate / (1.0 + jnp.exp(-gate))) * up

    def full_block(i):
        both = product(i, 2 * LANES)
        return activated(both[:, :LANES] * factor, both[:, LANES:] * factor).astype(BF16)

    def pair(p, carry):
        for j in range(2):
            gate_copy(2 * p + j).wait()
            hidden[p, :, j * LANES : (j + 1) * LANES] = full_block(2 * p + j)
        return carry

    lax.fori_loop(0, blocks // 2 - 1, pair, 0)
    last = blocks // 2 - 1
    gate_copy(blocks - 2).wait()
    hidden[last, :, :LANES] = full_block(blocks - 2)
    gate_copy(blocks - 1).wait()
    both = product(blocks - 1, LANES) * factor
    lane = lax.broadcasted_iota(jnp.int32, both.shape, 1)
    turned = pltpu.roll(both, LANES // 2, 1)
    hidden[last, :, LANES:] = jnp.where(lane < LANES // 2, activated(both, turned), 0.0).astype(BF16)
    for chip in range(chips):
        down_copy(chip).wait()
        total = jnp.zeros((length, width), F32)
        for p in range(blocks // 2):
            total += dot_t(hidden[p], down[chip, :, p * 2 * LANES : (p + 1) * 2 * LANES])
        partial[chip] = total.astype(BF16)


def down_kernel(scal, hidden, weight, partial, down, dsems):
    core = scal[0]
    chips, length, width = partial.shape

    def down_copy(chip):
        row = pl.multiple_of((chip * CORES + core) * width, width)
        return pltpu.make_async_copy(
            weight.at[pl.ds(row, width), pl.ds(weight.shape[1] - down.shape[2], down.shape[2])],
            down.at[chip],
            dsems.at[chip],
        )

    for chip in range(chips):
        down_copy(chip).start()
    for chip in range(chips):
        down_copy(chip).wait()
        total = jnp.zeros((length, width), F32)
        for p in range(hidden.shape[0]):
            total += dot_t(hidden[p], down[chip, :, p * 2 * LANES : (p + 1) * 2 * LANES])
        partial[chip] = total


def call(kernel, outs, flops, moved, in_specs, scratch=()):
    return pl.pallas_call(
        kernel,
        out_shape=outs,
        in_specs=in_specs,
        out_specs=jax.tree.map(lambda _: spec(), outs),
        scratch_shapes=list(scratch),
        cost_estimate=pl.CostEstimate(flops=flops, bytes_accessed=moved, transcendentals=0),
    )


def swap(array):
    return lax.ppermute(array, "core", [(0, 1), (1, 0)])


def local(
    tokens,
    norm_gain,
    in_weight,
    pool_weight,
    pool_scale,
    out_weight,
    ffn_gain,
    gate_weight,
    up_weight,
    down_weight,
):
    _, length, width = tokens.shape
    rows, units = gate_weight.shape
    core = lax.axis_index("core")
    chips = lax.axis_size("x")
    group = lax.axis_index("x") * CORES + core
    scal = jnp.stack([core, jnp.left_shift(1, group % 4)]).astype(jnp.int32)
    smem = spec(pltpu.SMEM)

    whole = units // LANES
    columns = []
    for i in range(whole):
        columns += [a[:, i * LANES : (i + 1) * LANES] for a in (gate_weight, up_weight)]
    columns += [a[:, whole * LANES :] for a in (gate_weight, up_weight)]
    columns += [down_weight.T, jnp.zeros((rows, LANES - units % LANES), BF16)]
    weight = lax.all_gather(jnp.concatenate(columns, axis=1), "fs", axis=0, tiled=True)

    gains = jnp.stack(pieces(norm_gain) + pieces(ffn_gain)).astype(BF16)
    sent = jnp.concatenate(
        [tokens[0], gains, jnp.zeros((EXTRA - gains.shape[0], width), BF16)], axis=0
    )
    own = lax.all_gather(sent, "x", axis=0)
    other = swap(own)
    in_full = lax.all_gather(in_weight, "fs", axis=0, tiled=True)
    out_full = lax.all_gather(out_weight, "fs", axis=0, tiled=True)
    channels = in_full.shape[1]
    pooled = call(
        mixer_kernel,
        jax.ShapeDtypeStruct((length, channels), BF16),
        2 * length * D * channels,
        6 * length * D,
        [smem] + [spec()] * 5,
    )(scal, own, other, in_full, pool_weight, pool_scale.reshape(1, -1))
    pooled_all = lax.all_gather(pooled, ("x", "core"), axis=0)
    mixed, scaled = call(
        out_kernel,
        (
            jax.ShapeDtypeStruct((length, width), F32),
            jax.ShapeDtypeStruct((length, width), BF16),
        ),
        2 * length * width * out_full.shape[0],
        4 * length * D,
        [spec()] * 4,
    )(pooled_all, out_full, tokens[0], ffn_gain.reshape(1, -1))
    own_two = lax.all_gather(scaled, "x", axis=0)
    other_two = swap(own_two)
    scale_two = call(
        square_kernel,
        jax.ShapeDtypeStruct((length, LANES), F32),
        6 * length * D,
        2 * length * D,
        [spec()] * 4,
    )(own_two, other_two, own[:, length:], other[:, length:])

    blocks = (units + LANES - 1) // LANES
    depth = blocks * LANES
    down_scratch = (
        VM((chips, width, depth), BF16),
        pltpu.SemaphoreType.DMA((chips,)),
    )
    anywhere = spec(pl.ANY)
    hidden, partial_other = call(
        hidden_kernel,
        (
            jax.ShapeDtypeStruct((blocks // 2, length, 2 * LANES), BF16),
            jax.ShapeDtypeStruct((chips, length, width), BF16),
        ),
        5 * length * D * units,
        4 * D * units,
        [smem, spec(), spec(), spec(), anywhere],
        (
            VM((blocks, D, 2 * LANES), BF16),
            down_scratch[0],
            pltpu.SemaphoreType.DMA((blocks,)),
            down_scratch[1],
        ),
    )(scal, own_two, other_two, scale_two, weight)
    arrived = swap(partial_other)
    partial_own = call(
        down_kernel,
        jax.ShapeDtypeStruct((chips, length, width), F32),
        length * D * units,
        D * units,
        [smem, spec(), anywhere],
        down_scratch,
    )(scal, hidden, weight)
    paired = (partial_own + arrived.astype(F32)).astype(BF16)
    summed = lax.all_to_all(paired, "x", split_axis=0, concat_axis=0, tiled=True)
    return (mixed + summed.astype(F32).sum(axis=0)).astype(BF16)[None]


def solution(mesh):
    sizes = mesh.devices.shape
    fine = Mesh(
        mesh.devices.reshape(*sizes[:2], sizes[2] // CORES, CORES), ("grp", "fs", "x", "core")
    )
    tp = ("x", "core")
    return jax.shard_map(
        local,
        mesh=fine,
        in_specs=(
            P(("grp", "fs"), None, tp),
            P(tp),
            P("fs", tp),
            P(tp, None, None),
            P(tp),
            P("fs", tp),
            P(tp),
            P("fs", tp),
            P("fs", tp),
            P(tp, "fs"),
        ),
        out_specs=P(("grp", "fs"), None, tp),
        check_vma=False,
    )
```

```python
import jax
import jax.numpy as jnp
from jax import lax
from jax.experimental import pallas as pl
from jax.experimental.pallas import tpu as pltpu
from jax.sharding import Mesh
from jax.sharding import PartitionSpec as P

D = 2048
GD = 128
EPSILON = 0.05
CORES = 2
LANES = 128
EXTRA = 16
VM = pltpu.VMEM
F32, BF16 = jnp.float32, jnp.bfloat16


def dot(a, b):
    return lax.dot_general(a, b, (((1,), (0,)), ((), ())), preferred_element_type=F32)


def dot_t(a, b):
    return lax.dot_general(a, b, (((1,), (1,)), ((), ())), preferred_element_type=F32)


def pack_kernel(*refs):
    count = 6
    weight, sent, sems = refs[count], refs[count + 1], refs[-1]
    copies = [
        pltpu.make_async_copy(source, target, sems.at[i])
        for i, (source, target) in enumerate(zip(refs[:count], refs[count + 2 : -1]))
    ]
    for copy in copies:
        copy.start()
    for copy in copies:
        copy.wait()
    tokens, norm_gain, ffn_gain, gate, up, down = refs[count + 2 : -1]
    units = gate.shape[1]
    whole = units // LANES
    for i in range(whole):
        weight[:, 2 * i * LANES : (2 * i + 1) * LANES] = gate[:, i * LANES : (i + 1) * LANES]
        weight[:, (2 * i + 1) * LANES : (2 * i + 2) * LANES] = up[:, i * LANES : (i + 1) * LANES]
    at = 2 * units
    weight[:, 2 * whole * LANES : at] = jnp.concatenate(
        [gate[:, whole * LANES :], up[:, whole * LANES :]], axis=1
    )
    weight[:, at : at + whole * LANES] = down[:, : whole * LANES]
    rest = down[:, whole * LANES :]
    weight[:, at + whole * LANES :] = jnp.concatenate([rest, jnp.zeros_like(rest)], axis=1)
    length = tokens.shape[0]
    sent[:length, :] = tokens[...]
    rows = []
    for gain in (norm_gain[...], ffn_gain[...]):
        high = gain.astype(BF16).astype(F32)
        mid = (gain - high).astype(BF16).astype(F32)
        rows += [high, mid, gain - high - mid]
    rows.append(jnp.zeros((EXTRA - len(rows), tokens.shape[1]), F32))
    sent[length:, :] = jnp.concatenate(rows, axis=0).astype(BF16)


def gain_row(block, at):
    rows = block[at : at + 3, :].astype(F32)
    return rows[0:1] + rows[1:2] + rows[2:3]


def spec(where=VM):
    return pl.BlockSpec(memory_space=where)


def mixer_kernel(scal, own, other, mine, theirs, pool_weight, pool_scale, pooled, weight):
    core, half_width = scal[0], scal[1]

    @pl.when(scal[2] == 0)
    def _():
        weight[...] = mine[...]

    @pl.when(scal[2] != 0)
    def _():
        weight[...] = theirs[...]

    chips = own.shape[0]
    length, width = own.shape[1] - EXTRA, own.shape[2]
    square = jnp.zeros((length, 1), F32)
    for side in (own, other):
        for chip in range(chips):
            part = side[chip, :length, :].astype(F32)
            square += jnp.sum(part * part, axis=1, keepdims=True)
    scale = lax.rsqrt(square / D + EPSILON)
    total = jnp.zeros((length, weight.shape[1]), F32)
    for which, side in ((core, own), (1 - core, other)):
        for chip in range(chips):
            gain = gain_row(side[chip, length:, :], 0)
            part = side[chip, :length, :].astype(F32)
            normed = (part * scale * gain).astype(BF16)
            row = pl.multiple_of((chip * CORES + which) * width, width)
            total += dot(normed, weight[pl.ds(row, width), :])
    pool_input = total.astype(BF16)
    row = lax.broadcasted_iota(jnp.int32, (length, length), 0)
    column = lax.broadcasted_iota(jnp.int32, (length, length), 1)
    inside = (column >= row - half_width) & (column < row + half_width)
    window = dot(inside.astype(F32).astype(BF16), pool_input)
    at = lax.broadcasted_iota(jnp.int32, (length, 1), 0)
    count = jnp.minimum(at + half_width, length) - jnp.maximum(at - half_width, 0)
    deviation = (window / count.astype(F32) - pool_input.astype(F32)).astype(BF16)
    mapped = dot(deviation, pool_weight[0])
    pooled[...] = (mapped * pool_scale[...]).astype(BF16)


def out_kernel(scal, pooled, mine, theirs, tokens, gain, mixed, scaled, weight):
    half = tokens.shape[1] // 2
    blocks, _, depth = pooled.shape
    shard = mine.shape[1] // 2

    def lay(source):
        for side in range(2):
            rows = source[:, side * shard : (side + 1) * shard, :]
            weight[:, side * half : (side + 1) * half] = rows.reshape(-1, half)

    @pl.when(scal[2] == 0)
    def _():
        lay(theirs)

    @pl.when(scal[2] != 0)
    def _():
        lay(mine)

    add = jnp.zeros(tokens.shape, F32)
    for block in range(blocks):
        add += dot(pooled[block], weight[block * depth : (block + 1) * depth, :])
    total = tokens[...].astype(F32) + add
    mixed[...] = total
    scaled[...] = (total * gain[...]).astype(BF16)


def square_kernel(scal, own, other, own_gain, other_gain, scale, features):
    core = scal[0]
    chips, length, width = own.shape
    square = jnp.zeros((length, 1), F32)
    for which, side, gains in ((core, own, own_gain), (1 - core, other, other_gain)):
        for chip in range(chips):
            gain = gain_row(gains[chip, length:, :], 3)
            block = side[chip]
            column = pl.multiple_of((chip * CORES + which) * width, width)
            features[:, pl.ds(column, width)] = block
            part = block.astype(F32)
            square += jnp.sum(part * part * (1.0 / (gain * gain)), axis=1, keepdims=True)
    scale[...] = jnp.broadcast_to(lax.rsqrt(square / D + EPSILON), scale.shape)


def hidden_kernel(scal, features_at, scale, weight, hidden, partial, features, wide, down, sems, dsems):
    core = scal[0]
    chips, length, width = partial.shape
    blocks = wide.shape[0]

    def gate_copy(i):
        return pltpu.make_async_copy(
            weight.at[:, pl.ds(i * 2 * LANES, 2 * LANES)], wide.at[i], sems.at[i]
        )

    def down_copy(chip):
        row = pl.multiple_of((chip * CORES + 1 - core) * width, width)
        return pltpu.make_async_copy(
            weight.at[pl.ds(row, width), pl.ds(weight.shape[1] - down.shape[2], down.shape[2])],
            down.at[chip],
            dsems.at[chip],
        )

    feature_copy = pltpu.make_async_copy(features_at, features, sems.at[blocks])
    feature_copy.start()
    for i in range(blocks):
        gate_copy(i).start()
    for chip in range(chips):
        down_copy(chip).start()
    factor = scale[...]
    feature_copy.wait()

    def product(i, columns):
        return dot(features[...], wide[i, :, :columns])

    def activated(gate, up):
        return (gate / (1.0 + jnp.exp(-gate))) * up

    def full_block(i):
        both = product(i, 2 * LANES)
        return activated(both[:, :LANES] * factor, both[:, LANES:] * factor).astype(BF16)

    def pair(p, carry):
        for j in range(2):
            gate_copy(2 * p + j).wait()
            hidden[p, :, j * LANES : (j + 1) * LANES] = full_block(2 * p + j)
        return carry

    lax.fori_loop(0, blocks // 2 - 1, pair, 0)
    last = blocks // 2 - 1
    gate_copy(blocks - 2).wait()
    hidden[last, :, :LANES] = full_block(blocks - 2)
    gate_copy(blocks - 1).wait()
    both = product(blocks - 1, LANES) * factor
    lane = lax.broadcasted_iota(jnp.int32, both.shape, 1)
    turned = pltpu.roll(both, LANES // 2, 1)
    hidden[last, :, LANES:] = jnp.where(lane < LANES // 2, activated(both, turned), 0.0).astype(BF16)
    for chip in range(chips):
        down_copy(chip).wait()
        total = jnp.zeros((length, width), F32)
        for p in range(blocks // 2):
            total += dot_t(hidden[p], down[chip, :, p * 2 * LANES : (p + 1) * 2 * LANES])
        partial[chip] = total.astype(BF16)


def down_kernel(scal, hidden, weight, partial, down, dsems):
    core = scal[0]
    chips, length, width = partial.shape

    def down_copy(chip):
        row = pl.multiple_of((chip * CORES + core) * width, width)
        return pltpu.make_async_copy(
            weight.at[pl.ds(row, width), pl.ds(weight.shape[1] - down.shape[2], down.shape[2])],
            down.at[chip],
            dsems.at[chip],
        )

    for chip in range(chips):
        down_copy(chip).start()
    for chip in range(chips):
        down_copy(chip).wait()
        total = jnp.zeros((length, width), F32)
        for p in range(hidden.shape[0]):
            total += dot_t(hidden[p], down[chip, :, p * 2 * LANES : (p + 1) * 2 * LANES])
        partial[chip] = total


def call(kernel, outs, flops, moved, in_specs, scratch=(), vmem=12):
    return pl.pallas_call(
        kernel,
        out_shape=outs,
        in_specs=in_specs,
        out_specs=jax.tree.map(lambda _: spec(), outs),
        scratch_shapes=list(scratch),
        compiler_params=pltpu.CompilerParams(vmem_limit_bytes=vmem << 20),
        cost_estimate=pl.CostEstimate(flops=flops, bytes_accessed=moved, transcendentals=0),
    )


def swap(array):
    return lax.ppermute(array, "core", [(0, 1), (1, 0)])


def local(
    tokens,
    norm_gain,
    in_weight,
    pool_weight,
    pool_scale,
    out_weight,
    ffn_gain,
    gate_weight,
    up_weight,
    down_weight,
):
    _, length, width = tokens.shape
    rows, units = gate_weight.shape
    core = lax.axis_index("core")
    chips = lax.axis_size("x")
    group = lax.axis_index("x") * CORES + core
    partner = lax.axis_index("grp") % 2
    scal = jnp.stack([core, jnp.left_shift(1, group % 4), partner]).astype(jnp.int32)
    smem = spec(pltpu.SMEM)
    anywhere = spec(pl.ANY)
    blocks = (units + LANES - 1) // LANES
    depth = blocks * LANES

    unpacked = (
        tokens[0],
        norm_gain.reshape(1, -1),
        ffn_gain.reshape(1, -1),
        gate_weight,
        up_weight,
        down_weight.T,
    )
    packed, sent = call(
        pack_kernel,
        (
            jax.ShapeDtypeStruct((rows, 2 * units + depth), BF16),
            jax.ShapeDtypeStruct((length + EXTRA, width), BF16),
        ),
        0,
        8 * rows * units,
        [anywhere] * 6,
        [VM(a.shape, a.dtype) for a in unpacked] + [pltpu.SemaphoreType.DMA((6,))],
        63,
    )(*unpacked)
    weight = lax.all_gather(packed, "fs", axis=0, tiled=True)

    own = lax.all_gather(sent, "x", axis=0)
    other = swap(own)

    channels = in_weight.shape[1]
    out_turned = jnp.concatenate(jnp.split(out_weight, width // channels, axis=1), axis=0)
    chosen = jnp.where(partner == 0, in_weight, out_turned)
    mine = lax.all_gather(chosen, "fs", axis=0, tiled=True)
    groups = lax.axis_size("grp")
    theirs = lax.ppermute(mine, "grp", [(i, i ^ 1) for i in range(groups)])
    pooled = call(
        mixer_kernel,
        jax.ShapeDtypeStruct((length, channels), BF16),
        2 * length * D * channels,
        6 * length * D,
        [smem] + [spec()] * 6,
        (VM(mine.shape, BF16),),
    )(scal, own, other, mine, theirs, pool_weight, pool_scale.reshape(1, -1))
    pooled_all = lax.all_gather(pooled, ("x", "core"), axis=0)
    by_shard = (-1, out_turned.shape[0], channels)
    mixed, scaled = call(
        out_kernel,
        (
            jax.ShapeDtypeStruct((length, width), F32),
            jax.ShapeDtypeStruct((length, width), BF16),
        ),
        2 * length * width * pooled_all.shape[0] * channels,
        4 * length * D,
        [smem] + [spec()] * 5,
        (VM((pooled_all.shape[0] * channels, width), BF16),),
    )(
        scal,
        pooled_all,
        mine.reshape(by_shard),
        theirs.reshape(by_shard),
        tokens[0],
        ffn_gain.reshape(1, -1),
    )
    own_two = lax.all_gather(scaled, "x", axis=0)
    other_two = swap(own_two)
    scale_two, features = call(
        square_kernel,
        (
            jax.ShapeDtypeStruct((length, LANES), F32),
            jax.ShapeDtypeStruct((length, chips * CORES * width), BF16),
        ),
        6 * length * D,
        4 * length * D,
        [smem] + [spec()] * 4,
    )(scal, own_two, other_two, own, other)

    down_scratch = (
        VM((chips, width, depth), BF16),
        pltpu.SemaphoreType.DMA((chips,)),
    )
    hidden, partial_other = call(
        hidden_kernel,
        (
            jax.ShapeDtypeStruct((blocks // 2, length, 2 * LANES), BF16),
            jax.ShapeDtypeStruct((chips, length, width), BF16),
        ),
        5 * length * D * units,
        4 * D * units,
        [smem, anywhere, spec(), anywhere],
        (
            VM(features.shape, BF16),
            VM((blocks, D, 2 * LANES), BF16),
            down_scratch[0],
            pltpu.SemaphoreType.DMA((blocks + 1,)),
            down_scratch[1],
        ),
        56,
    )(scal, features, scale_two, weight)
    arrived = swap(partial_other)
    partial_own = call(
        down_kernel,
        jax.ShapeDtypeStruct((chips, length, width), F32),
        length * D * units,
        D * units,
        [smem, spec(), anywhere],
        down_scratch,
        56,
    )(scal, hidden, weight)
    paired = (partial_own + arrived.astype(F32)).astype(BF16)
    summed = lax.all_to_all(paired, "x", split_axis=0, concat_axis=0, tiled=True)
    return (mixed + summed.astype(F32).sum(axis=0)).astype(BF16)[None]


def solution(mesh):
    sizes = mesh.devices.shape
    fine = Mesh(
        mesh.devices.reshape(*sizes[:2], sizes[2] // CORES, CORES), ("grp", "fs", "x", "core")
    )
    tp = ("x", "core")
    return jax.shard_map(
        local,
        mesh=fine,
        in_specs=(
            P(("grp", "fs"), None, tp),
            P(tp),
            P("fs", tp),
            P(tp, None, None),
            P(tp),
            P("fs", tp),
            P(tp),
            P("fs", tp),
            P("fs", tp),
            P(tp, "fs"),
        ),
        out_specs=P(("grp", "fs"), None, tp),
        check_vma=False,
    )
```

```python
import jax
import jax.numpy as jnp
from jax import lax
from jax.experimental import pallas as pl
from jax.experimental.pallas import tpu as pltpu
from jax.sharding import Mesh
from jax.sharding import PartitionSpec as P

D = 2048
GD = 128
EPSILON = 0.05
CORES = 2
LANES = 128
EXTRA = 16
VM = pltpu.VMEM
HIDDEN_VMEM = 50
F32, BF16 = jnp.float32, jnp.bfloat16


def dot(a, b):
    return lax.dot_general(a, b, (((1,), (0,)), ((), ())), preferred_element_type=F32)


def dot_t(a, b):
    return lax.dot_general(a, b, (((1,), (1,)), ((), ())), preferred_element_type=F32)


def pack_kernel(*refs):
    count = 6
    weight, sent, sems = refs[count], refs[count + 1], refs[-1]
    copies = [
        pltpu.make_async_copy(source, target, sems.at[i])
        for i, (source, target) in enumerate(zip(refs[:count], refs[count + 2 : -1]))
    ]
    for copy in copies:
        copy.start()
    for copy in copies:
        copy.wait()
    tokens, norm_gain, ffn_gain, gate, up, down = refs[count + 2 : -1]
    units = gate.shape[1]
    whole = units // LANES
    for i in range(whole):
        weight[:, 2 * i * LANES : (2 * i + 1) * LANES] = gate[:, i * LANES : (i + 1) * LANES]
        weight[:, (2 * i + 1) * LANES : (2 * i + 2) * LANES] = up[:, i * LANES : (i + 1) * LANES]
    at = 2 * units
    weight[:, 2 * whole * LANES : at] = jnp.concatenate(
        [gate[:, whole * LANES :], up[:, whole * LANES :]], axis=1
    )
    weight[:, at : at + whole * LANES] = down[:, : whole * LANES]
    rest = down[:, whole * LANES :]
    weight[:, at + whole * LANES :] = jnp.concatenate([rest, jnp.zeros_like(rest)], axis=1)
    length = tokens.shape[0]
    sent[:length, :] = tokens[...]
    rows = []
    for gain in (norm_gain[...], ffn_gain[...]):
        high = gain.astype(BF16).astype(F32)
        mid = (gain - high).astype(BF16).astype(F32)
        rows += [high, mid, gain - high - mid]
    rows.append(jnp.zeros((EXTRA - len(rows), tokens.shape[1]), F32))
    sent[length:, :] = jnp.concatenate(rows, axis=0).astype(BF16)


def gain_row(block, at):
    rows = block[at : at + 3, :].astype(F32)
    return rows[0:1] + rows[1:2] + rows[2:3]


def spec(where=VM):
    return pl.BlockSpec(memory_space=where)


def mixer_kernel(scal, own, other, mine, theirs, pool_weight, pool_scale, pooled, weight):
    core, half_width = scal[0], scal[1]

    @pl.when(scal[2] == 0)
    def _():
        weight[...] = mine[...]

    @pl.when(scal[2] != 0)
    def _():
        weight[...] = theirs[...]

    chips = own.shape[0]
    length, width = own.shape[1] - EXTRA, own.shape[2]
    square = jnp.zeros((length, 1), F32)
    for side in (own, other):
        for chip in range(chips):
            part = side[chip, :length, :].astype(F32)
            square += jnp.sum(part * part, axis=1, keepdims=True)
    scale = lax.rsqrt(square / D + EPSILON)
    total = jnp.zeros((length, weight.shape[1]), F32)
    for which, side in ((core, own), (1 - core, other)):
        for chip in range(chips):
            gain = gain_row(side[chip, length:, :], 0)
            part = side[chip, :length, :].astype(F32)
            normed = (part * scale * gain).astype(BF16)
            row = pl.multiple_of((chip * CORES + which) * width, width)
            total += dot(normed, weight[pl.ds(row, width), :])
    pool_input = total.astype(BF16)
    row = lax.broadcasted_iota(jnp.int32, (length, length), 0)
    column = lax.broadcasted_iota(jnp.int32, (length, length), 1)
    inside = (column >= row - half_width) & (column < row + half_width)
    window = dot(inside.astype(F32).astype(BF16), pool_input)
    at = lax.broadcasted_iota(jnp.int32, (length, 1), 0)
    count = jnp.minimum(at + half_width, length) - jnp.maximum(at - half_width, 0)
    deviation = (window / count.astype(F32) - pool_input.astype(F32)).astype(BF16)
    mapped = dot(deviation, pool_weight[0])
    pooled[...] = (mapped * pool_scale[...]).astype(BF16)


def out_kernel(scal, pooled, mine, theirs, tokens, gain, mixed, scaled, weight):
    half = tokens.shape[1] // 2
    blocks, _, depth = pooled.shape
    shard = mine.shape[1] // 2

    def lay(source):
        for side in range(2):
            rows = source[:, side * shard : (side + 1) * shard, :]
            weight[:, side * half : (side + 1) * half] = rows.reshape(-1, half)

    @pl.when(scal[2] == 0)
    def _():
        lay(theirs)

    @pl.when(scal[2] != 0)
    def _():
        lay(mine)

    add = jnp.zeros(tokens.shape, F32)
    for block in range(blocks):
        add += dot(pooled[block], weight[block * depth : (block + 1) * depth, :])
    total = tokens[...].astype(F32) + add
    mixed[...] = total
    scaled[...] = (total * gain[...]).astype(BF16)


def square_kernel(scal, own, other, own_gain, other_gain, scale, features):
    core = scal[0]
    chips, length, width = own.shape
    square = jnp.zeros((length, 1), F32)
    for which, side, gains in ((core, own, own_gain), (1 - core, other, other_gain)):
        for chip in range(chips):
            gain = gain_row(gains[chip, length:, :], 3)
            block = side[chip]
            column = pl.multiple_of((chip * CORES + which) * width, width)
            features[:, pl.ds(column, width)] = block
            part = block.astype(F32)
            square += jnp.sum(part * part * (1.0 / (gain * gain)), axis=1, keepdims=True)
    scale[...] = jnp.broadcast_to(lax.rsqrt(square / D + EPSILON), scale.shape)


def hidden_kernel(scal, features_at, scale, weight, hidden, partial, kept, features, wide, down, sems, dsems):
    core = scal[0]
    chips, length, width = partial.shape
    blocks = wide.shape[0]

    def gate_copy(i):
        return pltpu.make_async_copy(
            weight.at[:, pl.ds(i * 2 * LANES, 2 * LANES)], wide.at[i], sems.at[i]
        )

    def down_copy(chip, mine=False):
        row = pl.multiple_of((chip * CORES + (core if mine else 1 - core)) * width, width)
        return pltpu.make_async_copy(
            weight.at[pl.ds(row, width), pl.ds(weight.shape[1] - down.shape[2], down.shape[2])],
            (kept if mine else down).at[chip],
            dsems.at[chips + chip if mine else chip],
        )

    feature_copy = pltpu.make_async_copy(features_at, features, sems.at[blocks])
    feature_copy.start()
    for i in range(blocks):
        gate_copy(i).start()
    for chip in range(chips):
        down_copy(chip).start()
    for chip in range(chips):
        down_copy(chip, True).start()
    factor = scale[...]
    feature_copy.wait()

    def product(i, columns):
        return dot(features[...], wide[i, :, :columns])

    def activated(gate, up):
        return (gate / (1.0 + jnp.exp(-gate))) * up

    def full_block(i):
        both = product(i, 2 * LANES)
        return activated(both[:, :LANES] * factor, both[:, LANES:] * factor).astype(BF16)

    def pair(p, carry):
        for j in range(2):
            gate_copy(2 * p + j).wait()
            hidden[p, :, j * LANES : (j + 1) * LANES] = full_block(2 * p + j)
        return carry

    lax.fori_loop(0, blocks // 2 - 1, pair, 0)
    last = blocks // 2 - 1
    gate_copy(blocks - 2).wait()
    hidden[last, :, :LANES] = full_block(blocks - 2)
    gate_copy(blocks - 1).wait()
    both = product(blocks - 1, LANES) * factor
    lane = lax.broadcasted_iota(jnp.int32, both.shape, 1)
    turned = pltpu.roll(both, LANES // 2, 1)
    hidden[last, :, LANES:] = jnp.where(lane < LANES // 2, activated(both, turned), 0.0).astype(BF16)
    for chip in range(chips):
        down_copy(chip).wait()
        total = jnp.zeros((length, width), F32)
        for p in range(blocks // 2):
            total += dot_t(hidden[p], down[chip, :, p * 2 * LANES : (p + 1) * 2 * LANES])
        partial[chip] = total.astype(BF16)
    for chip in range(chips):
        down_copy(chip, True).wait()


def down_kernel(hidden, down, partial):
    for chip in range(partial.shape[0]):
        total = jnp.zeros(partial.shape[1:], F32)
        for p in range(hidden.shape[0]):
            total += dot_t(hidden[p], down[chip, :, p * 2 * LANES : (p + 1) * 2 * LANES])
        partial[chip] = total


def call(kernel, outs, flops, moved, in_specs, scratch=(), vmem=12):
    return pl.pallas_call(
        kernel,
        out_shape=outs,
        in_specs=in_specs,
        out_specs=jax.tree.map(lambda _: spec(), outs),
        scratch_shapes=list(scratch),
        compiler_params=pltpu.CompilerParams(vmem_limit_bytes=vmem << 20),
        cost_estimate=pl.CostEstimate(flops=flops, bytes_accessed=moved, transcendentals=0),
    )


def swap(array):
    return lax.ppermute(array, "core", [(0, 1), (1, 0)])


def local(
    tokens,
    norm_gain,
    in_weight,
    pool_weight,
    pool_scale,
    out_weight,
    ffn_gain,
    gate_weight,
    up_weight,
    down_weight,
):
    _, length, width = tokens.shape
    rows, units = gate_weight.shape
    core = lax.axis_index("core")
    chips = lax.axis_size("x")
    group = lax.axis_index("x") * CORES + core
    partner = lax.axis_index("grp") % 2
    scal = jnp.stack([core, jnp.left_shift(1, group % 4), partner]).astype(jnp.int32)
    smem = spec(pltpu.SMEM)
    anywhere = spec(pl.ANY)
    blocks = (units + LANES - 1) // LANES
    depth = blocks * LANES

    unpacked = (
        tokens[0],
        norm_gain.reshape(1, -1),
        ffn_gain.reshape(1, -1),
        gate_weight,
        up_weight,
        down_weight.T,
    )
    packed, sent = call(
        pack_kernel,
        (
            jax.ShapeDtypeStruct((rows, 2 * units + depth), BF16),
            jax.ShapeDtypeStruct((length + EXTRA, width), BF16),
        ),
        0,
        8 * rows * units,
        [anywhere] * 6,
        [VM(a.shape, a.dtype) for a in unpacked] + [pltpu.SemaphoreType.DMA((6,))],
        63,
    )(*unpacked)
    weight = lax.all_gather(packed, "fs", axis=0, tiled=True)

    own = lax.all_gather(sent, "x", axis=0)
    other = swap(own)

    channels = in_weight.shape[1]
    out_turned = jnp.concatenate(jnp.split(out_weight, width // channels, axis=1), axis=0)
    chosen = jnp.where(partner == 0, in_weight, out_turned)
    mine = lax.all_gather(chosen, "fs", axis=0, tiled=True)
    groups = lax.axis_size("grp")
    theirs = lax.ppermute(mine, "grp", [(i, i ^ 1) for i in range(groups)])
    pooled = call(
        mixer_kernel,
        jax.ShapeDtypeStruct((length, channels), BF16),
        2 * length * D * channels,
        6 * length * D,
        [smem] + [spec()] * 6,
        (VM(mine.shape, BF16),),
    )(scal, own, other, mine, theirs, pool_weight, pool_scale.reshape(1, -1))
    pooled_all = lax.all_gather(pooled, ("x", "core"), axis=0)
    by_shard = (-1, out_turned.shape[0], channels)
    mixed, scaled = call(
        out_kernel,
        (
            jax.ShapeDtypeStruct((length, width), F32),
            jax.ShapeDtypeStruct((length, width), BF16),
        ),
        2 * length * width * pooled_all.shape[0] * channels,
        4 * length * D,
        [smem] + [spec()] * 5,
        (VM((pooled_all.shape[0] * channels, width), BF16),),
    )(
        scal,
        pooled_all,
        mine.reshape(by_shard),
        theirs.reshape(by_shard),
        tokens[0],
        ffn_gain.reshape(1, -1),
    )
    own_two = lax.all_gather(scaled, "x", axis=0)
    other_two = swap(own_two)
    scale_two, features = call(
        square_kernel,
        (
            jax.ShapeDtypeStruct((length, LANES), F32),
            jax.ShapeDtypeStruct((length, chips * CORES * width), BF16),
        ),
        6 * length * D,
        4 * length * D,
        [smem] + [spec()] * 4,
    )(scal, own_two, other_two, own, other)

    hidden, partial_other, down_own = call(
        hidden_kernel,
        (
            jax.ShapeDtypeStruct((blocks // 2, length, 2 * LANES), BF16),
            jax.ShapeDtypeStruct((chips, length, width), BF16),
            jax.ShapeDtypeStruct((chips, width, depth), BF16),
        ),
        5 * length * D * units,
        6 * D * units,
        [smem, anywhere, spec(), anywhere],
        (
            VM(features.shape, BF16),
            VM((blocks, D, 2 * LANES), BF16),
            VM((chips, width, depth), BF16),
            pltpu.SemaphoreType.DMA((blocks + 1,)),
            pltpu.SemaphoreType.DMA((2 * chips,)),
        ),
        HIDDEN_VMEM,
    )(scal, features, scale_two, weight)
    arrived = swap(partial_other)
    partial_own = call(
        down_kernel,
        jax.ShapeDtypeStruct((chips, length, width), F32),
        length * D * units,
        D * units,
        [spec()] * 2,
    )(hidden, down_own)
    paired = (partial_own + arrived.astype(F32)).astype(BF16)
    summed = lax.all_to_all(paired, "x", split_axis=0, concat_axis=0, tiled=True)
    return (mixed + summed.astype(F32).sum(axis=0)).astype(BF16)[None]


def solution(mesh):
    sizes = mesh.devices.shape
    fine = Mesh(
        mesh.devices.reshape(*sizes[:2], sizes[2] // CORES, CORES), ("grp", "fs", "x", "core")
    )
    tp = ("x", "core")
    return jax.shard_map(
        local,
        mesh=fine,
        in_specs=(
            P(("grp", "fs"), None, tp),
            P(tp),
            P("fs", tp),
            P(tp, None, None),
            P(tp),
            P("fs", tp),
            P(tp),
            P("fs", tp),
            P("fs", tp),
            P(tp, "fs"),
        ),
        out_specs=P(("grp", "fs"), None, tp),
        check_vma=False,
    )
```

```python
import jax
import jax.numpy as jnp
from jax import lax
from jax.experimental import pallas as pl
from jax.experimental.pallas import tpu as pltpu
from jax.sharding import Mesh
from jax.sharding import PartitionSpec as P

D = 2048
GD = 128
EPSILON = 0.05
CORES = 2
LANES = 128
EXTRA = 16
VM = pltpu.VMEM
HIDDEN_VMEM = 50
F32, BF16 = jnp.float32, jnp.bfloat16


def dot(a, b):
    return lax.dot_general(a, b, (((1,), (0,)), ((), ())), preferred_element_type=F32)


def dot_t(a, b):
    return lax.dot_general(a, b, (((1,), (1,)), ((), ())), preferred_element_type=F32)


def pack_kernel(*refs):
    count = 6
    weight, sent, sems = refs[count], refs[count + 1], refs[-1]
    copies = [
        pltpu.make_async_copy(source, target, sems.at[i])
        for i, (source, target) in enumerate(zip(refs[:count], refs[count + 2 : -1]))
    ]
    for copy in copies:
        copy.start()
    for copy in copies:
        copy.wait()
    tokens, norm_gain, ffn_gain, gate, up, down = refs[count + 2 : -1]
    units = gate.shape[1]
    whole = units // LANES
    for i in range(whole):
        weight[:, 2 * i * LANES : (2 * i + 1) * LANES] = gate[:, i * LANES : (i + 1) * LANES]
        weight[:, (2 * i + 1) * LANES : (2 * i + 2) * LANES] = up[:, i * LANES : (i + 1) * LANES]
    at = 2 * units
    weight[:, 2 * whole * LANES : at] = jnp.concatenate(
        [gate[:, whole * LANES :], up[:, whole * LANES :]], axis=1
    )
    weight[:, at : at + whole * LANES] = down[:, : whole * LANES]
    rest = down[:, whole * LANES :]
    weight[:, at + whole * LANES :] = jnp.concatenate([rest, jnp.zeros_like(rest)], axis=1)
    length = tokens.shape[0]
    sent[:length, :] = tokens[...]
    rows = []
    for gain in (norm_gain[...], ffn_gain[...]):
        high = gain.astype(BF16).astype(F32)
        mid = (gain - high).astype(BF16).astype(F32)
        rows += [high, mid, gain - high - mid]
    rows.append(jnp.zeros((EXTRA - len(rows), tokens.shape[1]), F32))
    sent[length:, :] = jnp.concatenate(rows, axis=0).astype(BF16)


def gain_row(block, at):
    rows = block[at : at + 3, :].astype(F32)
    return rows[0:1] + rows[1:2] + rows[2:3]


def spec(where=VM):
    return pl.BlockSpec(memory_space=where)


def mixer_kernel(scal, own, other, mine, theirs, pool_weight, pool_scale, pooled, weight):
    core, half_width = scal[0], scal[1]

    @pl.when(scal[2] == 0)
    def _():
        weight[...] = mine[...]

    @pl.when(scal[2] != 0)
    def _():
        weight[...] = theirs[...]

    chips = own.shape[0]
    length, width = own.shape[1] - EXTRA, own.shape[2]
    square = jnp.zeros((length, 1), F32)
    for side in (own, other):
        for chip in range(chips):
            part = side[chip, :length, :].astype(F32)
            square += jnp.sum(part * part, axis=1, keepdims=True)
    scale = lax.rsqrt(square / D + EPSILON)
    total = jnp.zeros((length, weight.shape[1]), F32)
    for which, side in ((core, own), (1 - core, other)):
        for chip in range(chips):
            gain = gain_row(side[chip, length:, :], 0)
            part = side[chip, :length, :].astype(F32)
            normed = (part * scale * gain).astype(BF16)
            row = pl.multiple_of((chip * CORES + which) * width, width)
            total += dot(normed, weight[pl.ds(row, width), :])
    pool_input = total.astype(BF16)
    row = lax.broadcasted_iota(jnp.int32, (length, length), 0)
    column = lax.broadcasted_iota(jnp.int32, (length, length), 1)
    inside = (column >= row - half_width) & (column < row + half_width)
    window = dot(inside.astype(F32).astype(BF16), pool_input)
    at = lax.broadcasted_iota(jnp.int32, (length, 1), 0)
    count = jnp.minimum(at + half_width, length) - jnp.maximum(at - half_width, 0)
    deviation = (window / count.astype(F32) - pool_input.astype(F32)).astype(BF16)
    mapped = dot(deviation, pool_weight[0])
    pooled[...] = (mapped * pool_scale[...]).astype(BF16)


def out_kernel(scal, pooled, mine, theirs, tokens, gain, mixed, scaled, weight):
    half = tokens.shape[1] // 2
    blocks, _, depth = pooled.shape
    shard = mine.shape[1] // 2

    def lay(source):
        for side in range(2):
            rows = source[:, side * shard : (side + 1) * shard, :]
            weight[:, side * half : (side + 1) * half] = rows.reshape(-1, half)

    @pl.when(scal[2] == 0)
    def _():
        lay(theirs)

    @pl.when(scal[2] != 0)
    def _():
        lay(mine)

    add = jnp.zeros(tokens.shape, F32)
    for block in range(blocks):
        add += dot(pooled[block], weight[block * depth : (block + 1) * depth, :])
    total = tokens[...].astype(F32) + add
    mixed[...] = total
    scaled[...] = (total * gain[...]).astype(BF16)


def square_kernel(scal, own, other, own_gain, other_gain, scale, features):
    core = scal[0]
    chips, length, width = own.shape
    square = jnp.zeros((length, 1), F32)
    for which, side, gains in ((core, own, own_gain), (1 - core, other, other_gain)):
        for chip in range(chips):
            gain = gain_row(gains[chip, length:, :], 3)
            block = side[chip]
            features[chip, :, pl.ds(pl.multiple_of(which * width, width), width)] = block
            part = block.astype(F32)
            square += jnp.sum(part * part * (1.0 / (gain * gain)), axis=1, keepdims=True)
    scale[...] = jnp.broadcast_to(lax.rsqrt(square / D + EPSILON), scale.shape)


def hidden_kernel(
    scal, features_at, scale, weight, hidden, partial, kept, features, wide, total, sems
):
    core = scal[0]
    chips, length, width = partial.shape
    bands, depth, _ = wide.shape
    gated = total.shape[1]

    def band_copy(band):
        row = pl.multiple_of(band * depth, depth)
        return pltpu.make_async_copy(
            weight.at[pl.ds(row, depth), :], wide.at[band], sems.at[band]
        )

    feature_copy = pltpu.make_async_copy(features_at, features, sems.at[bands])
    feature_copy.start()
    for band in range(bands):
        band_copy(band).start()
    factor = scale[...]
    feature_copy.wait()
    steps = [(at, min(2 * LANES, gated - at)) for at in range(0, gated, 2 * LANES)]

    def add_band(band, first):
        band_copy(band).wait()
        for at, size in steps:
            part = dot(features[band], wide[band, :, at : at + size])
            total[:, at : at + size] = part if first else total[:, at : at + size] + part

    add_band(0, True)

    def later(band, carry):
        add_band(band, False)
        return carry

    lax.fori_loop(1, bands, later, 0)

    def activated(gate, up):
        return (gate / (1.0 + jnp.exp(-gate))) * up

    for i, (at, size) in enumerate(steps):
        pair, side = divmod(i, 2)
        if size == 2 * LANES:
            gate = total[:, at : at + LANES] * factor
            value = activated(gate, total[:, at + LANES : at + size] * factor)
        else:
            both = total[:, at : at + size] * factor
            lane = lax.broadcasted_iota(jnp.int32, both.shape, 1)
            turned = pltpu.roll(both, LANES // 2, 1)
            value = jnp.where(lane < LANES // 2, activated(both, turned), 0.0)
        hidden[pair, :, side * LANES : (side + 1) * LANES] = value.astype(BF16)
    for chip in range(chips):
        theirs = pl.multiple_of((1 - core) * width, width)
        product = jnp.zeros((length, width), F32)
        for p in range(hidden.shape[0]):
            at = gated + p * 2 * LANES
            product += dot_t(hidden[p], wide[chip, pl.ds(theirs, width), at : at + 2 * LANES])
        partial[chip] = product.astype(BF16)
        kept[chip] = wide[chip, pl.ds(pl.multiple_of(core * width, width), width), gated:]


def down_kernel(hidden, down, partial):
    for chip in range(partial.shape[0]):
        total = jnp.zeros(partial.shape[1:], F32)
        for p in range(hidden.shape[0]):
            total += dot_t(hidden[p], down[chip, :, p * 2 * LANES : (p + 1) * 2 * LANES])
        partial[chip] = total


def call(kernel, outs, flops, moved, in_specs, scratch=(), vmem=12):
    return pl.pallas_call(
        kernel,
        out_shape=outs,
        in_specs=in_specs,
        out_specs=jax.tree.map(lambda _: spec(), outs),
        scratch_shapes=list(scratch),
        compiler_params=pltpu.CompilerParams(vmem_limit_bytes=vmem << 20),
        cost_estimate=pl.CostEstimate(flops=flops, bytes_accessed=moved, transcendentals=0),
    )


def swap(array):
    return lax.ppermute(array, "core", [(0, 1), (1, 0)])


def local(
    tokens,
    norm_gain,
    in_weight,
    pool_weight,
    pool_scale,
    out_weight,
    ffn_gain,
    gate_weight,
    up_weight,
    down_weight,
):
    _, length, width = tokens.shape
    rows, units = gate_weight.shape
    core = lax.axis_index("core")
    chips = lax.axis_size("x")
    group = lax.axis_index("x") * CORES + core
    partner = lax.axis_index("grp") % 2
    scal = jnp.stack([core, jnp.left_shift(1, group % 4), partner]).astype(jnp.int32)
    smem = spec(pltpu.SMEM)
    anywhere = spec(pl.ANY)
    blocks = (units + LANES - 1) // LANES
    depth = blocks * LANES

    unpacked = (
        tokens[0],
        norm_gain.reshape(1, -1),
        ffn_gain.reshape(1, -1),
        gate_weight,
        up_weight,
        down_weight.T,
    )
    packed, sent = call(
        pack_kernel,
        (
            jax.ShapeDtypeStruct((rows, 2 * units + depth), BF16),
            jax.ShapeDtypeStruct((length + EXTRA, width), BF16),
        ),
        0,
        8 * rows * units,
        [anywhere] * 6,
        [VM(a.shape, a.dtype) for a in unpacked] + [pltpu.SemaphoreType.DMA((6,))],
        63,
    )(*unpacked)
    weight = lax.all_gather(packed, "fs", axis=0, tiled=True)

    own = lax.all_gather(sent, "x", axis=0)
    other = swap(own)

    channels = in_weight.shape[1]
    out_turned = jnp.concatenate(jnp.split(out_weight, width // channels, axis=1), axis=0)
    chosen = jnp.where(partner == 0, in_weight, out_turned)
    mine = lax.all_gather(chosen, "fs", axis=0, tiled=True)
    groups = lax.axis_size("grp")
    theirs = lax.ppermute(mine, "grp", [(i, i ^ 1) for i in range(groups)])
    pooled = call(
        mixer_kernel,
        jax.ShapeDtypeStruct((length, channels), BF16),
        2 * length * D * channels,
        6 * length * D,
        [smem] + [spec()] * 6,
        (VM(mine.shape, BF16),),
    )(scal, own, other, mine, theirs, pool_weight, pool_scale.reshape(1, -1))
    pooled_all = lax.all_gather(pooled, ("x", "core"), axis=0)
    by_shard = (-1, out_turned.shape[0], channels)
    mixed, scaled = call(
        out_kernel,
        (
            jax.ShapeDtypeStruct((length, width), F32),
            jax.ShapeDtypeStruct((length, width), BF16),
        ),
        2 * length * width * pooled_all.shape[0] * channels,
        4 * length * D,
        [smem] + [spec()] * 5,
        (VM((pooled_all.shape[0] * channels, width), BF16),),
    )(
        scal,
        pooled_all,
        mine.reshape(by_shard),
        theirs.reshape(by_shard),
        tokens[0],
        ffn_gain.reshape(1, -1),
    )
    own_two = lax.all_gather(scaled, "x", axis=0)
    other_two = swap(own_two)
    scale_two, features = call(
        square_kernel,
        (
            jax.ShapeDtypeStruct((length, LANES), F32),
            jax.ShapeDtypeStruct((chips, length, CORES * width), BF16),
        ),
        6 * length * D,
        4 * length * D,
        [smem] + [spec()] * 4,
    )(scal, own_two, other_two, own, other)

    hidden, partial_other, down_own = call(
        hidden_kernel,
        (
            jax.ShapeDtypeStruct((blocks // 2, length, 2 * LANES), BF16),
            jax.ShapeDtypeStruct((chips, length, width), BF16),
            jax.ShapeDtypeStruct((chips, width, depth), BF16),
        ),
        5 * length * D * units,
        6 * D * units,
        [smem, anywhere, spec(), anywhere],
        (
            VM(features.shape, BF16),
            VM((chips, CORES * width, weight.shape[1]), BF16),
            VM((length, 2 * units), F32),
            pltpu.SemaphoreType.DMA((chips + 1,)),
        ),
        HIDDEN_VMEM,
    )(scal, features, scale_two, weight)
    arrived = swap(partial_other)
    partial_own = call(
        down_kernel,
        jax.ShapeDtypeStruct((chips, length, width), F32),
        length * D * units,
        D * units,
        [spec()] * 2,
    )(hidden, down_own)
    paired = (partial_own + arrived.astype(F32)).astype(BF16)
    summed = lax.all_to_all(paired, "x", split_axis=0, concat_axis=0, tiled=True)
    return (mixed + summed.astype(F32).sum(axis=0)).astype(BF16)[None]


def solution(mesh):
    sizes = mesh.devices.shape
    fine = Mesh(
        mesh.devices.reshape(*sizes[:2], sizes[2] // CORES, CORES), ("grp", "fs", "x", "core")
    )
    tp = ("x", "core")
    return jax.shard_map(
        local,
        mesh=fine,
        in_specs=(
            P(("grp", "fs"), None, tp),
            P(tp),
            P("fs", tp),
            P(tp, None, None),
            P(tp),
            P("fs", tp),
            P(tp),
            P("fs", tp),
            P("fs", tp),
            P(tp, "fs"),
        ),
        out_specs=P(("grp", "fs"), None, tp),
        check_vma=False,
    )
```

```python
import jax
import jax.numpy as jnp
from jax import lax
from jax.experimental import pallas as pl
from jax.experimental.pallas import tpu as pltpu
from jax.sharding import Mesh
from jax.sharding import PartitionSpec as P

D = 2048
GD = 128
EPSILON = 0.05
CORES = 2
LANES = 128
EXTRA = 16
VM = pltpu.VMEM
HIDDEN_VMEM = 50
F32, BF16 = jnp.float32, jnp.bfloat16


def dot(a, b):
    return lax.dot_general(a, b, (((1,), (0,)), ((), ())), preferred_element_type=F32)


def dot_t(a, b):
    return lax.dot_general(a, b, (((1,), (1,)), ((), ())), preferred_element_type=F32)


def pack_kernel(*refs):
    count = 6
    weight, sent, sems = refs[count], refs[count + 1], refs[-1]
    copies = [
        pltpu.make_async_copy(source, target, sems.at[i])
        for i, (source, target) in enumerate(zip(refs[:count], refs[count + 2 : -1]))
    ]
    for copy in copies:
        copy.start()
    for copy in copies:
        copy.wait()
    tokens, norm_gain, ffn_gain, gate, up, down = refs[count + 2 : -1]
    units = gate.shape[1]
    whole = units // LANES
    for i in range(whole):
        weight[:, 2 * i * LANES : (2 * i + 1) * LANES] = gate[:, i * LANES : (i + 1) * LANES]
        weight[:, (2 * i + 1) * LANES : (2 * i + 2) * LANES] = up[:, i * LANES : (i + 1) * LANES]
    at = 2 * units
    weight[:, 2 * whole * LANES : at] = jnp.concatenate(
        [gate[:, whole * LANES :], up[:, whole * LANES :]], axis=1
    )
    weight[:, at : at + whole * LANES] = down[:, : whole * LANES]
    rest = down[:, whole * LANES :]
    weight[:, at + whole * LANES :] = jnp.concatenate([rest, jnp.zeros_like(rest)], axis=1)
    length = tokens.shape[0]
    sent[:length, :] = tokens[...]
    rows = []
    for gain in (norm_gain[...], ffn_gain[...]):
        high = gain.astype(BF16).astype(F32)
        mid = (gain - high).astype(BF16).astype(F32)
        rows += [high, mid, gain - high - mid]
    rows.append(jnp.zeros((EXTRA - len(rows), tokens.shape[1]), F32))
    sent[length:, :] = jnp.concatenate(rows, axis=0).astype(BF16)


def gain_row(block, at):
    rows = block[at : at + 3, :].astype(F32)
    return rows[0:1] + rows[1:2] + rows[2:3]


def spec(where=VM):
    return pl.BlockSpec(memory_space=where)


def mixer_kernel(scal, own, other, mine, theirs, pool_weight, pool_scale, pooled, weight):
    core, half_width = scal[0], scal[1]

    @pl.when(scal[2] == 0)
    def _():
        weight[...] = mine[...]

    @pl.when(scal[2] != 0)
    def _():
        weight[...] = theirs[...]

    chips = own.shape[0]
    length, width = own.shape[1] - EXTRA, own.shape[2]
    square = jnp.zeros((length, 1), F32)
    for side in (own, other):
        for chip in range(chips):
            part = side[chip, :length, :].astype(F32)
            square += jnp.sum(part * part, axis=1, keepdims=True)
    scale = lax.rsqrt(square / D + EPSILON)
    total = jnp.zeros((length, weight.shape[1]), F32)
    for which, side in ((core, own), (1 - core, other)):
        for chip in range(chips):
            gain = gain_row(side[chip, length:, :], 0)
            part = side[chip, :length, :].astype(F32)
            normed = (part * scale * gain).astype(BF16)
            row = pl.multiple_of((chip * CORES + which) * width, width)
            total += dot(normed, weight[pl.ds(row, width), :])
    pool_input = total.astype(BF16)
    row = lax.broadcasted_iota(jnp.int32, (length, length), 0)
    column = lax.broadcasted_iota(jnp.int32, (length, length), 1)
    inside = (column >= row - half_width) & (column < row + half_width)
    window = dot(inside.astype(F32).astype(BF16), pool_input)
    at = lax.broadcasted_iota(jnp.int32, (length, 1), 0)
    count = jnp.minimum(at + half_width, length) - jnp.maximum(at - half_width, 0)
    deviation = (window / count.astype(F32) - pool_input.astype(F32)).astype(BF16)
    mapped = dot(deviation, pool_weight[0])
    pooled[...] = (mapped * pool_scale[...]).astype(BF16)


def out_kernel(scal, pooled, mine, theirs, tokens, gain, mixed, scaled, weight):
    half = tokens.shape[1] // 2
    blocks, _, depth = pooled.shape
    shard = mine.shape[1] // 2

    def lay(source):
        for side in range(2):
            rows = source[:, side * shard : (side + 1) * shard, :]
            weight[:, side * half : (side + 1) * half] = rows.reshape(-1, half)

    @pl.when(scal[2] == 0)
    def _():
        lay(theirs)

    @pl.when(scal[2] != 0)
    def _():
        lay(mine)

    add = jnp.zeros(tokens.shape, F32)
    for block in range(blocks):
        add += dot(pooled[block], weight[block * depth : (block + 1) * depth, :])
    total = tokens[...].astype(F32) + add
    mixed[...] = total
    scaled[...] = (total * gain[...]).astype(BF16)


def square_kernel(scal, own, other, own_gain, other_gain, scale, features):
    core = scal[0]
    chips, length, width = own.shape
    square = jnp.zeros((length, 1), F32)
    for which, side, gains in ((core, own, own_gain), (1 - core, other, other_gain)):
        for chip in range(chips):
            gain = gain_row(gains[chip, length:, :], 3)
            block = side[chip]
            features[chip, :, pl.ds(pl.multiple_of(which * width, width), width)] = block
            part = block.astype(F32)
            square += jnp.sum(part * part * (1.0 / (gain * gain)), axis=1, keepdims=True)
    scale[...] = jnp.broadcast_to(lax.rsqrt(square / D + EPSILON), scale.shape)


def hidden_kernel(
    scal, features_at, scale, weight, hidden, partial, kept, features, wide, total, sems
):
    core = scal[0]
    chips, length, width = partial.shape
    bands, depth, _ = wide.shape
    gated = total.shape[1]

    def band_copy(band):
        row = pl.multiple_of(band * depth, depth)
        return pltpu.make_async_copy(
            weight.at[pl.ds(row, depth), :], wide.at[band], sems.at[band]
        )

    feature_copy = pltpu.make_async_copy(features_at, features, sems.at[bands])
    feature_copy.start()
    for band in range(bands):
        band_copy(band).start()
    factor = scale[...]
    feature_copy.wait()
    steps = [(at, min(2 * LANES, gated - at)) for at in range(0, gated, 2 * LANES)]

    def add_band(band, first):
        band_copy(band).wait()
        for at, size in steps:
            part = dot(features[band], wide[band, :, at : at + size])
            total[:, at : at + size] = part if first else total[:, at : at + size] + part

    add_band(0, True)

    def later(band, carry):
        add_band(band, False)
        return carry

    lax.fori_loop(1, bands, later, 0)

    def activated(gate, up):
        return (gate / (1.0 + jnp.exp(-gate))) * up

    for i, (at, size) in enumerate(steps):
        pair, side = divmod(i, 2)
        if size == 2 * LANES:
            gate = total[:, at : at + LANES] * factor
            value = activated(gate, total[:, at + LANES : at + size] * factor)
        else:
            both = total[:, at : at + size] * factor
            lane = lax.broadcasted_iota(jnp.int32, both.shape, 1)
            turned = pltpu.roll(both, LANES // 2, 1)
            value = jnp.where(lane < LANES // 2, activated(both, turned), 0.0)
        hidden[pair, :, side * LANES : (side + 1) * LANES] = value.astype(BF16)
    for chip in range(chips):
        theirs = pl.multiple_of((1 - core) * width, width)
        product = jnp.zeros((length, width), F32)
        for p in range(hidden.shape[0]):
            at = gated + p * 2 * LANES
            product += dot_t(hidden[p], wide[chip, pl.ds(theirs, width), at : at + 2 * LANES])
        partial[chip] = product.astype(BF16)
        kept[chip] = wide[chip, pl.ds(pl.multiple_of(core * width, width), width), gated:]


def down_kernel(hidden, down, partial):
    for chip in range(partial.shape[0]):
        total = jnp.zeros(partial.shape[1:], F32)
        for p in range(hidden.shape[0]):
            total += dot_t(hidden[p], down[chip, :, p * 2 * LANES : (p + 1) * 2 * LANES])
        partial[chip] = total


def call(kernel, outs, flops, moved, in_specs, scratch=(), vmem=12):
    return pl.pallas_call(
        kernel,
        out_shape=outs,
        in_specs=in_specs,
        out_specs=jax.tree.map(lambda _: spec(), outs),
        scratch_shapes=list(scratch),
        compiler_params=pltpu.CompilerParams(vmem_limit_bytes=vmem << 20),
        cost_estimate=pl.CostEstimate(flops=flops, bytes_accessed=moved, transcendentals=0),
    )


def swap(array):
    return lax.ppermute(array, "core", [(0, 1), (1, 0)])


def local(
    tokens,
    norm_gain,
    in_weight,
    pool_weight,
    pool_scale,
    out_weight,
    ffn_gain,
    gate_weight,
    up_weight,
    down_weight,
):
    _, length, width = tokens.shape
    rows, units = gate_weight.shape
    core = lax.axis_index("core")
    chips = lax.axis_size("x")
    group = lax.axis_index("x") * CORES + core
    partner = lax.axis_index("grp") % 2
    scal = jnp.stack([core, jnp.left_shift(1, group % 4), partner]).astype(jnp.int32)
    smem = spec(pltpu.SMEM)
    anywhere = spec(pl.ANY)
    blocks = (units + LANES - 1) // LANES
    depth = blocks * LANES

    unpacked = (
        tokens[0],
        norm_gain.reshape(1, -1),
        ffn_gain.reshape(1, -1),
        gate_weight,
        up_weight,
        down_weight.T,
    )
    packed, sent = call(
        pack_kernel,
        (
            jax.ShapeDtypeStruct((rows, 2 * units + depth), BF16),
            jax.ShapeDtypeStruct((length + EXTRA, width), BF16),
        ),
        0,
        8 * rows * units,
        [anywhere] * 6,
        [VM(a.shape, a.dtype) for a in unpacked] + [pltpu.SemaphoreType.DMA((6,))],
        63,
    )(*unpacked)
    length_fs = lax.axis_size("fs")
    place = [(z * CORES + c, z * CORES + (c + z) % CORES) for z in range(length_fs) for c in range(CORES)]
    packed = lax.ppermute(packed, ("fs", "core"), place)
    rings = [
        [(z * chips + x) * CORES + (c + z) % CORES for z in range(length_fs)]
        for x in range(chips)
        for c in range(CORES)
    ]
    weight = lax.all_gather(
        packed, ("fs", "x", "core"), axis=0, tiled=True, axis_index_groups=rings
    )

    own = lax.all_gather(sent, "x", axis=0)
    other = swap(own)

    channels = in_weight.shape[1]
    out_turned = jnp.concatenate(jnp.split(out_weight, width // channels, axis=1), axis=0)
    chosen = jnp.where(partner == 0, in_weight, out_turned)
    mine = lax.all_gather(chosen, "fs", axis=0, tiled=True)
    groups = lax.axis_size("grp")
    theirs = lax.ppermute(mine, "grp", [(i, i ^ 1) for i in range(groups)])
    pooled = call(
        mixer_kernel,
        jax.ShapeDtypeStruct((length, channels), BF16),
        2 * length * D * channels,
        6 * length * D,
        [smem] + [spec()] * 6,
        (VM(mine.shape, BF16),),
    )(scal, own, other, mine, theirs, pool_weight, pool_scale.reshape(1, -1))
    pooled_all = lax.all_gather(pooled, ("x", "core"), axis=0)
    by_shard = (-1, out_turned.shape[0], channels)
    mixed, scaled = call(
        out_kernel,
        (
            jax.ShapeDtypeStruct((length, width), F32),
            jax.ShapeDtypeStruct((length, width), BF16),
        ),
        2 * length * width * pooled_all.shape[0] * channels,
        4 * length * D,
        [smem] + [spec()] * 5,
        (VM((pooled_all.shape[0] * channels, width), BF16),),
    )(
        scal,
        pooled_all,
        mine.reshape(by_shard),
        theirs.reshape(by_shard),
        tokens[0],
        ffn_gain.reshape(1, -1),
    )
    own_two = lax.all_gather(scaled, "x", axis=0)
    other_two = swap(own_two)
    scale_two, features = call(
        square_kernel,
        (
            jax.ShapeDtypeStruct((length, LANES), F32),
            jax.ShapeDtypeStruct((chips, length, CORES * width), BF16),
        ),
        6 * length * D,
        4 * length * D,
        [smem] + [spec()] * 4,
    )(scal, own_two, other_two, own, other)

    hidden, partial_other, down_own = call(
        hidden_kernel,
        (
            jax.ShapeDtypeStruct((blocks // 2, length, 2 * LANES), BF16),
            jax.ShapeDtypeStruct((chips, length, width), BF16),
            jax.ShapeDtypeStruct((chips, width, depth), BF16),
        ),
        5 * length * D * units,
        6 * D * units,
        [smem, anywhere, spec(), anywhere],
        (
            VM(features.shape, BF16),
            VM((chips, CORES * width, weight.shape[1]), BF16),
            VM((length, 2 * units), F32),
            pltpu.SemaphoreType.DMA((chips + 1,)),
        ),
        HIDDEN_VMEM,
    )(scal, features, scale_two, weight)
    arrived = swap(partial_other)
    partial_own = call(
        down_kernel,
        jax.ShapeDtypeStruct((chips, length, width), F32),
        length * D * units,
        D * units,
        [spec()] * 2,
    )(hidden, down_own)
    paired = (partial_own + arrived.astype(F32)).astype(BF16)
    summed = lax.all_to_all(paired, "x", split_axis=0, concat_axis=0, tiled=True)
    return (mixed + summed.astype(F32).sum(axis=0)).astype(BF16)[None]


def solution(mesh):
    sizes = mesh.devices.shape
    fine = Mesh(
        mesh.devices.reshape(*sizes[:2], sizes[2] // CORES, CORES), ("grp", "fs", "x", "core")
    )
    tp = ("x", "core")
    return jax.shard_map(
        local,
        mesh=fine,
        in_specs=(
            P(("grp", "fs"), None, tp),
            P(tp),
            P("fs", tp),
            P(tp, None, None),
            P(tp),
            P("fs", tp),
            P(tp),
            P("fs", tp),
            P("fs", tp),
            P(tp, "fs"),
        ),
        out_specs=P(("grp", "fs"), None, tp),
        check_vma=False,
    )
```

```python
import jax
import jax.numpy as jnp
from jax import lax
from jax.experimental import pallas as pl
from jax.experimental.pallas import tpu as pltpu
from jax.sharding import Mesh
from jax.sharding import PartitionSpec as P

D = 2048
GD = 128
EPSILON = 0.05
CORES = 2
LANES = 128
EXTRA = 16
VM = pltpu.VMEM
HIDDEN_VMEM = 50
F32, BF16 = jnp.float32, jnp.bfloat16


def dot(a, b):
    return lax.dot_general(a, b, (((1,), (0,)), ((), ())), preferred_element_type=F32)


def dot_t(a, b):
    return lax.dot_general(a, b, (((1,), (1,)), ((), ())), preferred_element_type=F32)


def pack_kernel(*refs):
    count = 6
    weight, sent, sems = refs[count], refs[count + 1], refs[-1]
    copies = [
        pltpu.make_async_copy(source, target, sems.at[i])
        for i, (source, target) in enumerate(zip(refs[:count], refs[count + 2 : -1]))
    ]
    for copy in copies:
        copy.start()
    for copy in copies:
        copy.wait()
    tokens, norm_gain, ffn_gain, gate, up, down = refs[count + 2 : -1]
    units = gate.shape[1]
    whole = units // LANES
    for i in range(whole):
        weight[:, 2 * i * LANES : (2 * i + 1) * LANES] = gate[:, i * LANES : (i + 1) * LANES]
        weight[:, (2 * i + 1) * LANES : (2 * i + 2) * LANES] = up[:, i * LANES : (i + 1) * LANES]
    at = 2 * units
    weight[:, 2 * whole * LANES : at] = jnp.concatenate(
        [gate[:, whole * LANES :], up[:, whole * LANES :]], axis=1
    )
    weight[:, at : at + whole * LANES] = down[:, : whole * LANES]
    rest = down[:, whole * LANES :]
    weight[:, at + whole * LANES :] = jnp.concatenate([rest, jnp.zeros_like(rest)], axis=1)
    length = tokens.shape[0]
    sent[:length, :] = tokens[...]
    rows = []
    for gain in (norm_gain[...], ffn_gain[...]):
        high = gain.astype(BF16).astype(F32)
        mid = (gain - high).astype(BF16).astype(F32)
        rows += [high, mid, gain - high - mid]
    rows.append(jnp.zeros((EXTRA - len(rows), tokens.shape[1]), F32))
    sent[length:, :] = jnp.concatenate(rows, axis=0).astype(BF16)


def gain_row(block, at):
    rows = block[at : at + 3, :].astype(F32)
    return rows[0:1] + rows[1:2] + rows[2:3]


def spec(where=VM):
    return pl.BlockSpec(memory_space=where)


def mixer_kernel(scal, own, other, mine, theirs, pool_weight, pool_scale, pooled, weight):
    core, half_width = scal[0], scal[1]

    @pl.when(scal[2] == 0)
    def _():
        weight[...] = mine[...]

    @pl.when(scal[2] != 0)
    def _():
        weight[...] = theirs[...]

    chips = own.shape[0]
    length, width = own.shape[1] - EXTRA, own.shape[2]
    square = jnp.zeros((length, 1), F32)
    for side in (own, other):
        for chip in range(chips):
            part = side[chip, :length, :].astype(F32)
            square += jnp.sum(part * part, axis=1, keepdims=True)
    scale = lax.rsqrt(square / D + EPSILON)
    total = jnp.zeros((length, weight.shape[1]), F32)
    for which, side in ((core, own), (1 - core, other)):
        for chip in range(chips):
            gain = gain_row(side[chip, length:, :], 0)
            part = side[chip, :length, :].astype(F32)
            normed = (part * scale * gain).astype(BF16)
            row = pl.multiple_of((chip * CORES + which) * width, width)
            total += dot(normed, weight[pl.ds(row, width), :])
    pool_input = total.astype(BF16)
    row = lax.broadcasted_iota(jnp.int32, (length, length), 0)
    column = lax.broadcasted_iota(jnp.int32, (length, length), 1)
    inside = (column >= row - half_width) & (column < row + half_width)
    window = dot(inside.astype(F32).astype(BF16), pool_input)
    at = lax.broadcasted_iota(jnp.int32, (length, 1), 0)
    count = jnp.minimum(at + half_width, length) - jnp.maximum(at - half_width, 0)
    deviation = (window / count.astype(F32) - pool_input.astype(F32)).astype(BF16)
    mapped = dot(deviation, pool_weight[0])
    pooled[...] = (mapped * pool_scale[...]).astype(BF16)


def out_kernel(scal, pooled, mine, theirs, tokens, gain, mixed, scaled, weight):
    half = tokens.shape[1] // 2
    blocks, _, depth = pooled.shape
    shard = mine.shape[1] // 2

    def lay(source):
        for side in range(2):
            rows = source[:, side * shard : (side + 1) * shard, :]
            weight[:, side * half : (side + 1) * half] = rows.reshape(-1, half)

    @pl.when(scal[2] == 0)
    def _():
        lay(theirs)

    @pl.when(scal[2] != 0)
    def _():
        lay(mine)

    add = jnp.zeros(tokens.shape, F32)
    for block in range(blocks):
        add += dot(pooled[block], weight[block * depth : (block + 1) * depth, :])
    total = tokens[...].astype(F32) + add
    mixed[...] = total
    scaled[...] = (total * gain[...]).astype(BF16)


def square_kernel(scal, own, other, own_gain, other_gain, scale, features):
    core = scal[0]
    chips, length, width = own.shape
    square = jnp.zeros((length, 1), F32)
    for which, side, gains in ((core, own, own_gain), (1 - core, other, other_gain)):
        for chip in range(chips):
            gain = gain_row(gains[chip, length:, :], 3)
            block = side[chip]
            features[chip, :, pl.ds(pl.multiple_of(which * width, width), width)] = block
            part = block.astype(F32)
            square += jnp.sum(part * part * (1.0 / (gain * gain)), axis=1, keepdims=True)
    scale[...] = jnp.broadcast_to(lax.rsqrt(square / D + EPSILON), scale.shape)


def flips(core):
    return 0, 3 - 2 * core, 1 + 2 * core, 2


def hidden_kernel(
    scal, features_at, scale, weight, hidden, partial, kept, features, wide, total, sems
):
    core = scal[0]
    chips, length, width = partial.shape
    bands, depth, _ = wide.shape
    gated = total.shape[1]

    def band_copy(band):
        row = pl.multiple_of(band * depth, depth)
        return pltpu.make_async_copy(
            weight.at[pl.ds(row, depth), :], wide.at[band], sems.at[band]
        )

    feature_copy = pltpu.make_async_copy(features_at, features, sems.at[bands])
    feature_copy.start()
    for band in range(bands):
        band_copy(band).start()
    factor = scale[...]
    feature_copy.wait()
    steps = [(at, min(2 * LANES, gated - at)) for at in range(0, gated, 2 * LANES)]

    def add_band(band, first):
        band_copy(band).wait()
        for at, size in steps:
            part = dot(features[band], wide[band, :, at : at + size])
            total[:, at : at + size] = part if first else total[:, at : at + size] + part

    add_band(0, True)

    def later(band, carry):
        add_band(band, False)
        return carry

    lax.fori_loop(1, bands, later, 0)

    def activated(gate, up):
        return (gate / (1.0 + jnp.exp(-gate))) * up

    for i, (at, size) in enumerate(steps):
        pair, side = divmod(i, 2)
        if size == 2 * LANES:
            gate = total[:, at : at + LANES] * factor
            value = activated(gate, total[:, at + LANES : at + size] * factor)
        else:
            both = total[:, at : at + size] * factor
            lane = lax.broadcasted_iota(jnp.int32, both.shape, 1)
            turned = pltpu.roll(both, LANES // 2, 1)
            value = jnp.where(lane < LANES // 2, activated(both, turned), 0.0)
        hidden[pair, :, side * LANES : (side + 1) * LANES] = value.astype(BF16)
    theirs = pl.ds(pl.multiple_of((1 - core) * width, width), width)
    mine = pl.ds(pl.multiple_of(core * width, width), width)
    for place, flip in enumerate(flips(1 - core)):
        chip = jnp.bitwise_xor(scal[3], flip)
        product = jnp.zeros((length, width), F32)
        for p in range(hidden.shape[0]):
            at = gated + p * 2 * LANES
            product += dot_t(hidden[p], wide[chip, theirs, at : at + 2 * LANES])
        partial[place] = product.astype(BF16)
    for place, flip in enumerate(flips(core)):
        kept[place] = wide[jnp.bitwise_xor(scal[3], flip), mine, gated:]


def down_kernel(hidden, down, partial):
    for chip in range(partial.shape[0]):
        total = jnp.zeros(partial.shape[1:], F32)
        for p in range(hidden.shape[0]):
            total += dot_t(hidden[p], down[chip, :, p * 2 * LANES : (p + 1) * 2 * LANES])
        partial[chip] = total


def call(kernel, outs, flops, moved, in_specs, scratch=(), vmem=12):
    return pl.pallas_call(
        kernel,
        out_shape=outs,
        in_specs=in_specs,
        out_specs=jax.tree.map(lambda _: spec(), outs),
        scratch_shapes=list(scratch),
        compiler_params=pltpu.CompilerParams(vmem_limit_bytes=vmem << 20),
        cost_estimate=pl.CostEstimate(flops=flops, bytes_accessed=moved, transcendentals=0),
    )


def swap(array):
    return lax.ppermute(array, "core", [(0, 1), (1, 0)])


def local(
    tokens,
    norm_gain,
    in_weight,
    pool_weight,
    pool_scale,
    out_weight,
    ffn_gain,
    gate_weight,
    up_weight,
    down_weight,
):
    _, length, width = tokens.shape
    rows, units = gate_weight.shape
    core = lax.axis_index("core")
    chips = lax.axis_size("x")
    group = lax.axis_index("x") * CORES + core
    partner = lax.axis_index("grp") % 2
    scal = jnp.stack(
        [core, jnp.left_shift(1, group % 4), partner, lax.axis_index("x")]
    ).astype(jnp.int32)
    smem = spec(pltpu.SMEM)
    anywhere = spec(pl.ANY)
    blocks = (units + LANES - 1) // LANES
    depth = blocks * LANES

    unpacked = (
        tokens[0],
        norm_gain.reshape(1, -1),
        ffn_gain.reshape(1, -1),
        gate_weight,
        up_weight,
        down_weight.T,
    )
    packed, sent = call(
        pack_kernel,
        (
            jax.ShapeDtypeStruct((rows, 2 * units + depth), BF16),
            jax.ShapeDtypeStruct((length + EXTRA, width), BF16),
        ),
        0,
        8 * rows * units,
        [anywhere] * 6,
        [VM(a.shape, a.dtype) for a in unpacked] + [pltpu.SemaphoreType.DMA((6,))],
        63,
    )(*unpacked)
    length_fs = lax.axis_size("fs")
    place = [(z * CORES + c, z * CORES + (c + z) % CORES) for z in range(length_fs) for c in range(CORES)]
    packed = lax.ppermute(packed, ("fs", "core"), place)
    rings = [
        [(z * chips + x) * CORES + (c + z) % CORES for z in range(length_fs)]
        for x in range(chips)
        for c in range(CORES)
    ]
    weight = lax.all_gather(
        packed, ("fs", "x", "core"), axis=0, tiled=True, axis_index_groups=rings
    )

    own = lax.all_gather(sent, "x", axis=0)
    other = swap(own)

    channels = in_weight.shape[1]
    out_turned = jnp.concatenate(jnp.split(out_weight, width // channels, axis=1), axis=0)
    chosen = jnp.where(partner == 0, in_weight, out_turned)
    mine = lax.all_gather(chosen, "fs", axis=0, tiled=True)
    groups = lax.axis_size("grp")
    theirs = lax.ppermute(mine, "grp", [(i, i ^ 1) for i in range(groups)])
    pooled = call(
        mixer_kernel,
        jax.ShapeDtypeStruct((length, channels), BF16),
        2 * length * D * channels,
        6 * length * D,
        [smem] + [spec()] * 6,
        (VM(mine.shape, BF16),),
    )(scal, own, other, mine, theirs, pool_weight, pool_scale.reshape(1, -1))
    pooled_all = lax.all_gather(pooled, ("x", "core"), axis=0)
    by_shard = (-1, out_turned.shape[0], channels)
    mixed, scaled = call(
        out_kernel,
        (
            jax.ShapeDtypeStruct((length, width), F32),
            jax.ShapeDtypeStruct((length, width), BF16),
        ),
        2 * length * width * pooled_all.shape[0] * channels,
        4 * length * D,
        [smem] + [spec()] * 5,
        (VM((pooled_all.shape[0] * channels, width), BF16),),
    )(
        scal,
        pooled_all,
        mine.reshape(by_shard),
        theirs.reshape(by_shard),
        tokens[0],
        ffn_gain.reshape(1, -1),
    )
    own_two = lax.all_gather(scaled, "x", axis=0)
    other_two = swap(own_two)
    scale_two, features = call(
        square_kernel,
        (
            jax.ShapeDtypeStruct((length, LANES), F32),
            jax.ShapeDtypeStruct((chips, length, CORES * width), BF16),
        ),
        6 * length * D,
        4 * length * D,
        [smem] + [spec()] * 4,
    )(scal, own_two, other_two, own, other)

    hidden, partial_other, down_own = call(
        hidden_kernel,
        (
            jax.ShapeDtypeStruct((blocks // 2, length, 2 * LANES), BF16),
            jax.ShapeDtypeStruct((chips, length, width), BF16),
            jax.ShapeDtypeStruct((chips, width, depth), BF16),
        ),
        5 * length * D * units,
        6 * D * units,
        [smem, anywhere, spec(), anywhere],
        (
            VM(features.shape, BF16),
            VM((chips, CORES * width, weight.shape[1]), BF16),
            VM((length, 2 * units), F32),
            pltpu.SemaphoreType.DMA((chips + 1,)),
        ),
        HIDDEN_VMEM,
    )(scal, features, scale_two, weight)
    arrived = swap(partial_other)
    partial_own = call(
        down_kernel,
        jax.ShapeDtypeStruct((chips, length, width), F32),
        length * D * units,
        D * units,
        [spec()] * 2,
    )(hidden, down_own)
    def exchange(array, step):
        pairs = [
            (x * CORES + c, (x ^ flips(c)[step]) * CORES + c)
            for x in range(chips)
            for c in range(CORES)
        ]
        return lax.ppermute(array, ("x", "core"), pairs).astype(F32)

    paired = partial_own + arrived.astype(F32)
    halved = paired[:2] + exchange(paired[2:].astype(BF16), 2)
    last = exchange(halved[1].astype(BF16), 1)
    return (mixed + (halved[0] + last)).astype(BF16)[None]


def solution(mesh):
    sizes = mesh.devices.shape
    fine = Mesh(
        mesh.devices.reshape(*sizes[:2], sizes[2] // CORES, CORES), ("grp", "fs", "x", "core")
    )
    tp = ("x", "core")
    return jax.shard_map(
        local,
        mesh=fine,
        in_specs=(
            P(("grp", "fs"), None, tp),
            P(tp),
            P("fs", tp),
            P(tp, None, None),
            P(tp),
            P("fs", tp),
            P(tp),
            P("fs", tp),
            P("fs", tp),
            P(tp, "fs"),
        ),
        out_specs=P(("grp", "fs"), None, tp),
        check_vma=False,
    )
```

```python
import jax
import jax.numpy as jnp
from jax import lax
from jax.experimental import pallas as pl
from jax.experimental.pallas import tpu as pltpu
from jax.sharding import Mesh
from jax.sharding import PartitionSpec as P

D = 2048
GD = 128
EPSILON = 0.05
CORES = 2
LANES = 128
EXTRA = 16
VM = pltpu.VMEM
HIDDEN_VMEM = 50
F32, BF16 = jnp.float32, jnp.bfloat16


def dot(a, b):
    return lax.dot_general(a, b, (((1,), (0,)), ((), ())), preferred_element_type=F32)


def dot_t(a, b):
    return lax.dot_general(a, b, (((1,), (1,)), ((), ())), preferred_element_type=F32)


def pack_kernel(*refs):
    count = 6
    weight, sent, sems = refs[count], refs[count + 1], refs[-1]
    copies = [
        pltpu.make_async_copy(source, target, sems.at[i])
        for i, (source, target) in enumerate(zip(refs[:count], refs[count + 2 : -1]))
    ]
    for copy in copies:
        copy.start()
    for copy in copies:
        copy.wait()
    tokens, norm_gain, ffn_gain, gate, up, down = refs[count + 2 : -1]
    units = gate.shape[1]
    whole = units // LANES
    for i in range(whole):
        weight[:, 2 * i * LANES : (2 * i + 1) * LANES] = gate[:, i * LANES : (i + 1) * LANES]
        weight[:, (2 * i + 1) * LANES : (2 * i + 2) * LANES] = up[:, i * LANES : (i + 1) * LANES]
    at = 2 * units
    weight[:, 2 * whole * LANES : at] = jnp.concatenate(
        [gate[:, whole * LANES :], up[:, whole * LANES :]], axis=1
    )
    weight[:, at : at + whole * LANES] = down[:, : whole * LANES]
    rest = down[:, whole * LANES :]
    weight[:, at + whole * LANES :] = jnp.concatenate([rest, jnp.zeros_like(rest)], axis=1)
    length = tokens.shape[0]
    sent[:length, :] = tokens[...]
    rows = []
    for gain in (norm_gain[...], ffn_gain[...]):
        high = gain.astype(BF16).astype(F32)
        mid = (gain - high).astype(BF16).astype(F32)
        rows += [high, mid, gain - high - mid]
    rows.append(jnp.zeros((EXTRA - len(rows), tokens.shape[1]), F32))
    sent[length:, :] = jnp.concatenate(rows, axis=0).astype(BF16)


def gain_row(block, at):
    rows = block[at : at + 3, :].astype(F32)
    return rows[0:1] + rows[1:2] + rows[2:3]


def spec(where=VM):
    return pl.BlockSpec(memory_space=where)


def mixer_kernel(scal, own, other, mine, theirs, pool_weight, pool_scale, pooled, weight):
    core, half_width = scal[0], scal[1]

    @pl.when(scal[2] == 0)
    def _():
        weight[...] = mine[...]

    @pl.when(scal[2] != 0)
    def _():
        weight[...] = theirs[...]

    chips = own.shape[0]
    length, width = own.shape[1] - EXTRA, own.shape[2]
    square = jnp.zeros((length, 1), F32)
    for side in (own, other):
        for chip in range(chips):
            part = side[chip, :length, :].astype(F32)
            square += jnp.sum(part * part, axis=1, keepdims=True)
    scale = lax.rsqrt(square / D + EPSILON)
    total = jnp.zeros((length, weight.shape[1]), F32)
    for which, side in ((core, own), (1 - core, other)):
        for chip in range(chips):
            gain = gain_row(side[chip, length:, :], 0)
            part = side[chip, :length, :].astype(F32)
            normed = (part * scale * gain).astype(BF16)
            row = pl.multiple_of((chip * CORES + which) * width, width)
            total += dot(normed, weight[pl.ds(row, width), :])
    pool_input = total.astype(BF16)
    row = lax.broadcasted_iota(jnp.int32, (length, length), 0)
    column = lax.broadcasted_iota(jnp.int32, (length, length), 1)
    inside = (column >= row - half_width) & (column < row + half_width)
    window = dot(inside.astype(F32).astype(BF16), pool_input)
    at = lax.broadcasted_iota(jnp.int32, (length, 1), 0)
    count = jnp.minimum(at + half_width, length) - jnp.maximum(at - half_width, 0)
    deviation = (window / count.astype(F32) - pool_input.astype(F32)).astype(BF16)
    mapped = dot(deviation, pool_weight[0])
    pooled[...] = (mapped * pool_scale[...]).astype(BF16)


def out_kernel(scal, pooled, mine, theirs, tokens, gain, mixed, scaled, weight):
    half = tokens.shape[1] // 2
    blocks, _, depth = pooled.shape
    shard = mine.shape[1] // 2

    def lay(source):
        for side in range(2):
            rows = source[:, side * shard : (side + 1) * shard, :]
            weight[:, side * half : (side + 1) * half] = rows.reshape(-1, half)

    @pl.when(scal[2] == 0)
    def _():
        lay(theirs)

    @pl.when(scal[2] != 0)
    def _():
        lay(mine)

    add = jnp.zeros(tokens.shape, F32)
    for block in range(blocks):
        add += dot(pooled[block], weight[block * depth : (block + 1) * depth, :])
    total = tokens[...].astype(F32) + add
    mixed[...] = total
    scaled[...] = (total * gain[...]).astype(BF16)


def square_kernel(scal, own, other, own_gain, other_gain, scale, features):
    core = scal[0]
    chips, length, width = own.shape
    square = jnp.zeros((length, 1), F32)
    for which, side, gains in ((core, own, own_gain), (1 - core, other, other_gain)):
        for chip in range(chips):
            gain = gain_row(gains[chip, length:, :], 3)
            block = side[chip]
            features[chip, :, pl.ds(pl.multiple_of(which * width, width), width)] = block
            part = block.astype(F32)
            square += jnp.sum(part * part * (1.0 / (gain * gain)), axis=1, keepdims=True)
    scale[...] = jnp.broadcast_to(lax.rsqrt(square / D + EPSILON), scale.shape)


def hidden_kernel(
    scal, features_at, scale, weight, hidden, partial, kept, features, wide, total, sems
):
    core = scal[0]
    chips, length, width = partial.shape
    bands, depth, _ = wide.shape
    gated = total.shape[1]

    def band_copy(band):
        row = pl.multiple_of(band * depth, depth)
        return pltpu.make_async_copy(
            weight.at[pl.ds(row, depth), :], wide.at[band], sems.at[band]
        )

    feature_copy = pltpu.make_async_copy(features_at, features, sems.at[bands])
    feature_copy.start()
    for band in range(bands):
        band_copy(band).start()
    factor = scale[...]
    feature_copy.wait()
    steps = [(at, min(2 * LANES, gated - at)) for at in range(0, gated, 2 * LANES)]

    def add_band(band, first):
        band_copy(band).wait()
        for at, size in steps:
            part = dot(features[band], wide[band, :, at : at + size])
            total[:, at : at + size] = part if first else total[:, at : at + size] + part

    add_band(0, True)

    def later(band, carry):
        add_band(band, False)
        return carry

    lax.fori_loop(1, bands, later, 0)

    def activated(gate, up):
        return (gate / (1.0 + jnp.exp(-gate))) * up

    for i, (at, size) in enumerate(steps):
        pair, side = divmod(i, 2)
        if size == 2 * LANES:
            gate = total[:, at : at + LANES] * factor
            value = activated(gate, total[:, at + LANES : at + size] * factor)
        else:
            both = total[:, at : at + size] * factor
            lane = lax.broadcasted_iota(jnp.int32, both.shape, 1)
            turned = pltpu.roll(both, LANES // 2, 1)
            value = jnp.where(lane < LANES // 2, activated(both, turned), 0.0)
        hidden[pair, :, side * LANES : (side + 1) * LANES] = value.astype(BF16)
    theirs = pl.ds(pl.multiple_of((1 - core) * width, width), width)
    mine = pl.ds(pl.multiple_of(core * width, width), width)
    for place in range(chips):
        chip = lax.rem(scal[3] + place, chips)
        product = jnp.zeros((length, width), F32)
        for p in range(hidden.shape[0]):
            at = gated + p * 2 * LANES
            product += dot_t(hidden[p], wide[chip, theirs, at : at + 2 * LANES])
        partial[place] = product.astype(BF16)
        kept[place] = wide[chip, mine, gated:]


def down_kernel(hidden, down, partial):
    for chip in range(partial.shape[0]):
        total = jnp.zeros(partial.shape[1:], F32)
        for p in range(hidden.shape[0]):
            total += dot_t(hidden[p], down[chip, :, p * 2 * LANES : (p + 1) * 2 * LANES])
        partial[chip] = total


def call(kernel, outs, flops, moved, in_specs, scratch=(), vmem=12):
    return pl.pallas_call(
        kernel,
        out_shape=outs,
        in_specs=in_specs,
        out_specs=jax.tree.map(lambda _: spec(), outs),
        scratch_shapes=list(scratch),
        compiler_params=pltpu.CompilerParams(vmem_limit_bytes=vmem << 20),
        cost_estimate=pl.CostEstimate(flops=flops, bytes_accessed=moved, transcendentals=0),
    )


def swap(array):
    return lax.ppermute(array, "core", [(0, 1), (1, 0)])


def local(
    tokens,
    norm_gain,
    in_weight,
    pool_weight,
    pool_scale,
    out_weight,
    ffn_gain,
    gate_weight,
    up_weight,
    down_weight,
):
    _, length, width = tokens.shape
    rows, units = gate_weight.shape
    core = lax.axis_index("core")
    chips = lax.axis_size("x")
    group = lax.axis_index("x") * CORES + core
    partner = lax.axis_index("grp") % 2
    scal = jnp.stack(
        [core, jnp.left_shift(1, group % 4), partner, lax.axis_index("x")]
    ).astype(jnp.int32)
    smem = spec(pltpu.SMEM)
    anywhere = spec(pl.ANY)
    blocks = (units + LANES - 1) // LANES
    depth = blocks * LANES

    unpacked = (
        tokens[0],
        norm_gain.reshape(1, -1),
        ffn_gain.reshape(1, -1),
        gate_weight,
        up_weight,
        down_weight.T,
    )
    packed, sent = call(
        pack_kernel,
        (
            jax.ShapeDtypeStruct((rows, 2 * units + depth), BF16),
            jax.ShapeDtypeStruct((length + EXTRA, width), BF16),
        ),
        0,
        8 * rows * units,
        [anywhere] * 6,
        [VM(a.shape, a.dtype) for a in unpacked] + [pltpu.SemaphoreType.DMA((6,))],
        63,
    )(*unpacked)
    length_fs = lax.axis_size("fs")
    place = [(z * CORES + c, z * CORES + (c + z) % CORES) for z in range(length_fs) for c in range(CORES)]
    packed = lax.ppermute(packed, ("fs", "core"), place)
    rings = [
        [(z * chips + x) * CORES + (c + z) % CORES for z in range(length_fs)]
        for x in range(chips)
        for c in range(CORES)
    ]
    weight = lax.all_gather(
        packed, ("fs", "x", "core"), axis=0, tiled=True, axis_index_groups=rings
    )

    own = lax.all_gather(sent, "x", axis=0)
    other = swap(own)

    channels = in_weight.shape[1]
    out_turned = jnp.concatenate(jnp.split(out_weight, width // channels, axis=1), axis=0)
    chosen = jnp.where(partner == 0, in_weight, out_turned)
    mine = lax.all_gather(chosen, "fs", axis=0, tiled=True)
    groups = lax.axis_size("grp")
    theirs = lax.ppermute(mine, "grp", [(i, i ^ 1) for i in range(groups)])
    pooled = call(
        mixer_kernel,
        jax.ShapeDtypeStruct((length, channels), BF16),
        2 * length * D * channels,
        6 * length * D,
        [smem] + [spec()] * 6,
        (VM(mine.shape, BF16),),
    )(scal, own, other, mine, theirs, pool_weight, pool_scale.reshape(1, -1))
    pooled_all = lax.all_gather(pooled, ("x", "core"), axis=0)
    by_shard = (-1, out_turned.shape[0], channels)
    mixed, scaled = call(
        out_kernel,
        (
            jax.ShapeDtypeStruct((length, width), F32),
            jax.ShapeDtypeStruct((length, width), BF16),
        ),
        2 * length * width * pooled_all.shape[0] * channels,
        4 * length * D,
        [smem] + [spec()] * 5,
        (VM((pooled_all.shape[0] * channels, width), BF16),),
    )(
        scal,
        pooled_all,
        mine.reshape(by_shard),
        theirs.reshape(by_shard),
        tokens[0],
        ffn_gain.reshape(1, -1),
    )
    own_two = lax.all_gather(scaled, "x", axis=0)
    other_two = swap(own_two)
    scale_two, features = call(
        square_kernel,
        (
            jax.ShapeDtypeStruct((length, LANES), F32),
            jax.ShapeDtypeStruct((chips, length, CORES * width), BF16),
        ),
        6 * length * D,
        4 * length * D,
        [smem] + [spec()] * 4,
    )(scal, own_two, other_two, own, other)

    hidden, partial_other, down_own = call(
        hidden_kernel,
        (
            jax.ShapeDtypeStruct((blocks // 2, length, 2 * LANES), BF16),
            jax.ShapeDtypeStruct((chips, length, width), BF16),
            jax.ShapeDtypeStruct((chips, width, depth), BF16),
        ),
        5 * length * D * units,
        6 * D * units,
        [smem, anywhere, spec(), anywhere],
        (
            VM(features.shape, BF16),
            VM((chips, CORES * width, weight.shape[1]), BF16),
            VM((length, 2 * units), F32),
            pltpu.SemaphoreType.DMA((chips + 1,)),
        ),
        HIDDEN_VMEM,
    )(scal, features, scale_two, weight)
    arrived = swap(partial_other)
    partial_own = call(
        down_kernel,
        jax.ShapeDtypeStruct((chips, length, width), F32),
        length * D * units,
        D * units,
        [spec()] * 2,
    )(hidden, down_own)
    paired = partial_own + arrived.astype(F32)
    total = paired[0]
    for k in (1, chips - 1, *range(2, chips - 1)):
        onward = [(x, (x + k) % chips) for x in range(chips)]
        total = total + lax.ppermute(paired[k].astype(BF16), "x", onward).astype(F32)
    return (mixed + total).astype(BF16)[None]


def solution(mesh):
    sizes = mesh.devices.shape
    fine = Mesh(
        mesh.devices.reshape(*sizes[:2], sizes[2] // CORES, CORES), ("grp", "fs", "x", "core")
    )
    tp = ("x", "core")
    return jax.shard_map(
        local,
        mesh=fine,
        in_specs=(
            P(("grp", "fs"), None, tp),
            P(tp),
            P("fs", tp),
            P(tp, None, None),
            P(tp),
            P("fs", tp),
            P(tp),
            P("fs", tp),
            P("fs", tp),
            P(tp, "fs"),
        ),
        out_specs=P(("grp", "fs"), None, tp),
        check_vma=False,
    )
```

```python
import jax
import jax.numpy as jnp
from jax import lax
from jax.experimental import pallas as pl
from jax.experimental.pallas import tpu as pltpu
from jax.sharding import Mesh
from jax.sharding import PartitionSpec as P

D = 2048
GD = 128
EPSILON = 0.05
CORES = 2
LANES = 128
EXTRA = 16
VM = pltpu.VMEM
HIDDEN_VMEM = 50
F32, BF16 = jnp.float32, jnp.bfloat16


def dot(a, b):
    return lax.dot_general(a, b, (((1,), (0,)), ((), ())), preferred_element_type=F32)


def dot_t(a, b):
    return lax.dot_general(a, b, (((1,), (1,)), ((), ())), preferred_element_type=F32)


def pack_kernel(*refs):
    count = 6
    weight, sent, sems = refs[count], refs[count + 1], refs[-1]
    copies = [
        pltpu.make_async_copy(source, target, sems.at[i])
        for i, (source, target) in enumerate(zip(refs[:count], refs[count + 2 : -1]))
    ]
    for copy in copies:
        copy.start()
    for copy in copies:
        copy.wait()
    tokens, norm_gain, ffn_gain, gate, up, down = refs[count + 2 : -1]
    units = gate.shape[1]
    whole = units // LANES
    for i in range(whole):
        weight[:, 2 * i * LANES : (2 * i + 1) * LANES] = gate[:, i * LANES : (i + 1) * LANES]
        weight[:, (2 * i + 1) * LANES : (2 * i + 2) * LANES] = up[:, i * LANES : (i + 1) * LANES]
    at = 2 * units
    weight[:, 2 * whole * LANES : at] = jnp.concatenate(
        [gate[:, whole * LANES :], up[:, whole * LANES :]], axis=1
    )
    weight[:, at : at + whole * LANES] = down[:, : whole * LANES]
    rest = down[:, whole * LANES :]
    weight[:, at + whole * LANES :] = jnp.concatenate([rest, jnp.zeros_like(rest)], axis=1)
    length = tokens.shape[0]
    sent[:length, :] = tokens[...]
    rows = []
    for gain in (norm_gain[...], ffn_gain[...]):
        high = gain.astype(BF16).astype(F32)
        mid = (gain - high).astype(BF16).astype(F32)
        rows += [high, mid, gain - high - mid]
    rows.append(jnp.zeros((EXTRA - len(rows), tokens.shape[1]), F32))
    sent[length:, :] = jnp.concatenate(rows, axis=0).astype(BF16)


def gain_row(block, at):
    rows = block[at : at + 3, :].astype(F32)
    return rows[0:1] + rows[1:2] + rows[2:3]


def spec(where=VM):
    return pl.BlockSpec(memory_space=where)


def mixer_kernel(scal, own, other, mine, theirs, pool_weight, pool_scale, pooled, weight):
    core, half_width = scal[0], scal[1]

    @pl.when(scal[2] == 0)
    def _():
        weight[...] = mine[...]

    @pl.when(scal[2] != 0)
    def _():
        weight[...] = theirs[...]

    chips = own.shape[0]
    length, width = own.shape[1] - EXTRA, own.shape[2]
    square = jnp.zeros((length, 1), F32)
    for side in (own, other):
        for chip in range(chips):
            part = side[chip, :length, :].astype(F32)
            square += jnp.sum(part * part, axis=1, keepdims=True)
    scale = lax.rsqrt(square / D + EPSILON)
    total = jnp.zeros((length, weight.shape[1]), F32)
    for which, side in ((core, own), (1 - core, other)):
        for chip in range(chips):
            gain = gain_row(side[chip, length:, :], 0)
            part = side[chip, :length, :].astype(F32)
            normed = (part * scale * gain).astype(BF16)
            row = pl.multiple_of((chip * CORES + which) * width, width)
            total += dot(normed, weight[pl.ds(row, width), :])
    pool_input = total.astype(BF16)
    row = lax.broadcasted_iota(jnp.int32, (length, length), 0)
    column = lax.broadcasted_iota(jnp.int32, (length, length), 1)
    inside = (column >= row - half_width) & (column < row + half_width)
    window = dot(inside.astype(F32).astype(BF16), pool_input)
    at = lax.broadcasted_iota(jnp.int32, (length, 1), 0)
    count = jnp.minimum(at + half_width, length) - jnp.maximum(at - half_width, 0)
    deviation = (window / count.astype(F32) - pool_input.astype(F32)).astype(BF16)
    mapped = dot(deviation, pool_weight[0])
    pooled[...] = (mapped * pool_scale[...]).astype(BF16)


def out_kernel(scal, pooled, mine, theirs, tokens, gain, mixed, scaled, weight):
    half = tokens.shape[1] // 2
    blocks, _, depth = pooled.shape
    shard = mine.shape[1] // 2

    def lay(source):
        for side in range(2):
            rows = source[:, side * shard : (side + 1) * shard, :]
            weight[:, side * half : (side + 1) * half] = rows.reshape(-1, half)

    @pl.when(scal[2] == 0)
    def _():
        lay(theirs)

    @pl.when(scal[2] != 0)
    def _():
        lay(mine)

    add = jnp.zeros(tokens.shape, F32)
    for block in range(blocks):
        add += dot(pooled[block], weight[block * depth : (block + 1) * depth, :])
    total = tokens[...].astype(F32) + add
    mixed[...] = total
    scaled[...] = (total * gain[...]).astype(BF16)


def square_kernel(scal, own, other, own_gain, other_gain, scale, features):
    core = scal[0]
    chips, length, width = own.shape
    square = jnp.zeros((length, 1), F32)
    for which, side, gains in ((core, own, own_gain), (1 - core, other, other_gain)):
        for chip in range(chips):
            gain = gain_row(gains[chip, length:, :], 3)
            block = side[chip]
            features[chip, :, pl.ds(pl.multiple_of(which * width, width), width)] = block
            part = block.astype(F32)
            square += jnp.sum(part * part * (1.0 / (gain * gain)), axis=1, keepdims=True)
    scale[...] = jnp.broadcast_to(lax.rsqrt(square / D + EPSILON), scale.shape)


def hidden_kernel(
    scal, features_at, scale, weight, hidden, partial, kept, features, wide, total, sems
):
    core = scal[0]
    chips, length, width = partial.shape
    bands, depth, _ = wide.shape
    gated = total.shape[1]

    def band_copy(band, down=False):
        row = pl.multiple_of(band * depth, depth)
        columns = pl.ds(gated, weight.shape[1] - gated) if down else pl.ds(0, gated)
        return pltpu.make_async_copy(
            weight.at[pl.ds(row, depth), columns],
            wide.at[band, :, columns],
            sems.at[bands + band if down else band],
        )

    feature_copy = pltpu.make_async_copy(features_at, features, sems.at[2 * bands])
    feature_copy.start()
    for band in range(bands):
        band_copy(band).start()
    for band in range(bands):
        band_copy(band, True).start()
    factor = scale[...]
    feature_copy.wait()
    steps = [(at, min(2 * LANES, gated - at)) for at in range(0, gated, 2 * LANES)]

    def add_band(band, first):
        band_copy(band).wait()
        for at, size in steps:
            part = dot(features[band], wide[band, :, at : at + size])
            total[:, at : at + size] = part if first else total[:, at : at + size] + part

    add_band(0, True)

    def later(band, carry):
        add_band(band, False)
        return carry

    lax.fori_loop(1, bands, later, 0)

    def activated(gate, up):
        return (gate / (1.0 + jnp.exp(-gate))) * up

    for i, (at, size) in enumerate(steps):
        pair, side = divmod(i, 2)
        if size == 2 * LANES:
            gate = total[:, at : at + LANES] * factor
            value = activated(gate, total[:, at + LANES : at + size] * factor)
        else:
            both = total[:, at : at + size] * factor
            lane = lax.broadcasted_iota(jnp.int32, both.shape, 1)
            turned = pltpu.roll(both, LANES // 2, 1)
            value = jnp.where(lane < LANES // 2, activated(both, turned), 0.0)
        hidden[pair, :, side * LANES : (side + 1) * LANES] = value.astype(BF16)
    for chip in range(chips):
        band_copy(chip, True).wait()
        theirs = pl.multiple_of((1 - core) * width, width)
        product = jnp.zeros((length, width), F32)
        for p in range(hidden.shape[0]):
            at = gated + p * 2 * LANES
            product += dot_t(hidden[p], wide[chip, pl.ds(theirs, width), at : at + 2 * LANES])
        partial[chip] = product.astype(BF16)
        kept[chip] = wide[chip, pl.ds(pl.multiple_of(core * width, width), width), gated:]


def down_kernel(hidden, down, partial):
    for chip in range(partial.shape[0]):
        total = jnp.zeros(partial.shape[1:], F32)
        for p in range(hidden.shape[0]):
            total += dot_t(hidden[p], down[chip, :, p * 2 * LANES : (p + 1) * 2 * LANES])
        partial[chip] = total


def call(kernel, outs, flops, moved, in_specs, scratch=(), vmem=12):
    return pl.pallas_call(
        kernel,
        out_shape=outs,
        in_specs=in_specs,
        out_specs=jax.tree.map(lambda _: spec(), outs),
        scratch_shapes=list(scratch),
        compiler_params=pltpu.CompilerParams(vmem_limit_bytes=vmem << 20),
        cost_estimate=pl.CostEstimate(flops=flops, bytes_accessed=moved, transcendentals=0),
    )


def swap(array):
    return lax.ppermute(array, "core", [(0, 1), (1, 0)])


def local(
    tokens,
    norm_gain,
    in_weight,
    pool_weight,
    pool_scale,
    out_weight,
    ffn_gain,
    gate_weight,
    up_weight,
    down_weight,
):
    _, length, width = tokens.shape
    rows, units = gate_weight.shape
    core = lax.axis_index("core")
    chips = lax.axis_size("x")
    group = lax.axis_index("x") * CORES + core
    partner = lax.axis_index("grp") % 2
    scal = jnp.stack([core, jnp.left_shift(1, group % 4), partner]).astype(jnp.int32)
    smem = spec(pltpu.SMEM)
    anywhere = spec(pl.ANY)
    blocks = (units + LANES - 1) // LANES
    depth = blocks * LANES

    unpacked = (
        tokens[0],
        norm_gain.reshape(1, -1),
        ffn_gain.reshape(1, -1),
        gate_weight,
        up_weight,
        down_weight.T,
    )
    packed, sent = call(
        pack_kernel,
        (
            jax.ShapeDtypeStruct((rows, 2 * units + depth), BF16),
            jax.ShapeDtypeStruct((length + EXTRA, width), BF16),
        ),
        0,
        8 * rows * units,
        [anywhere] * 6,
        [VM(a.shape, a.dtype) for a in unpacked] + [pltpu.SemaphoreType.DMA((6,))],
        63,
    )(*unpacked)
    length_fs = lax.axis_size("fs")
    place = [(z * CORES + c, z * CORES + (c + z) % CORES) for z in range(length_fs) for c in range(CORES)]
    packed = lax.ppermute(packed, ("fs", "core"), place)
    rings = [
        [(z * chips + x) * CORES + (c + z) % CORES for z in range(length_fs)]
        for x in range(chips)
        for c in range(CORES)
    ]
    weight = lax.all_gather(
        packed, ("fs", "x", "core"), axis=0, tiled=True, axis_index_groups=rings
    )

    own = lax.all_gather(sent, "x", axis=0)
    other = swap(own)

    channels = in_weight.shape[1]
    out_turned = jnp.concatenate(jnp.split(out_weight, width // channels, axis=1), axis=0)
    chosen = jnp.where(partner == 0, in_weight, out_turned)
    mine = lax.all_gather(chosen, "fs", axis=0, tiled=True)
    groups = lax.axis_size("grp")
    theirs = lax.ppermute(mine, "grp", [(i, i ^ 1) for i in range(groups)])
    pooled = call(
        mixer_kernel,
        jax.ShapeDtypeStruct((length, channels), BF16),
        2 * length * D * channels,
        6 * length * D,
        [smem] + [spec()] * 6,
        (VM(mine.shape, BF16),),
    )(scal, own, other, mine, theirs, pool_weight, pool_scale.reshape(1, -1))
    pooled_all = lax.all_gather(pooled, ("x", "core"), axis=0)
    by_shard = (-1, out_turned.shape[0], channels)
    mixed, scaled = call(
        out_kernel,
        (
            jax.ShapeDtypeStruct((length, width), F32),
            jax.ShapeDtypeStruct((length, width), BF16),
        ),
        2 * length * width * pooled_all.shape[0] * channels,
        4 * length * D,
        [smem] + [spec()] * 5,
        (VM((pooled_all.shape[0] * channels, width), BF16),),
    )(
        scal,
        pooled_all,
        mine.reshape(by_shard),
        theirs.reshape(by_shard),
        tokens[0],
        ffn_gain.reshape(1, -1),
    )
    own_two = lax.all_gather(scaled, "x", axis=0)
    other_two = swap(own_two)
    scale_two, features = call(
        square_kernel,
        (
            jax.ShapeDtypeStruct((length, LANES), F32),
            jax.ShapeDtypeStruct((chips, length, CORES * width), BF16),
        ),
        6 * length * D,
        4 * length * D,
        [smem] + [spec()] * 4,
    )(scal, own_two, other_two, own, other)

    hidden, partial_other, down_own = call(
        hidden_kernel,
        (
            jax.ShapeDtypeStruct((blocks // 2, length, 2 * LANES), BF16),
            jax.ShapeDtypeStruct((chips, length, width), BF16),
            jax.ShapeDtypeStruct((chips, width, depth), BF16),
        ),
        5 * length * D * units,
        6 * D * units,
        [smem, anywhere, spec(), anywhere],
        (
            VM(features.shape, BF16),
            VM((chips, CORES * width, weight.shape[1]), BF16),
            VM((length, 2 * units), F32),
            pltpu.SemaphoreType.DMA((2 * chips + 1,)),
        ),
        HIDDEN_VMEM,
    )(scal, features, scale_two, weight)
    arrived = swap(partial_other)
    partial_own = call(
        down_kernel,
        jax.ShapeDtypeStruct((chips, length, width), F32),
        length * D * units,
        D * units,
        [spec()] * 2,
    )(hidden, down_own)
    paired = (partial_own + arrived.astype(F32)).astype(BF16)
    summed = lax.all_to_all(paired, "x", split_axis=0, concat_axis=0, tiled=True)
    return (mixed + summed.astype(F32).sum(axis=0)).astype(BF16)[None]


def solution(mesh):
    sizes = mesh.devices.shape
    fine = Mesh(
        mesh.devices.reshape(*sizes[:2], sizes[2] // CORES, CORES), ("grp", "fs", "x", "core")
    )
    tp = ("x", "core")
    return jax.shard_map(
        local,
        mesh=fine,
        in_specs=(
            P(("grp", "fs"), None, tp),
            P(tp),
            P("fs", tp),
            P(tp, None, None),
            P(tp),
            P("fs", tp),
            P(tp),
            P("fs", tp),
            P("fs", tp),
            P(tp, "fs"),
        ),
        out_specs=P(("grp", "fs"), None, tp),
        check_vma=False,
    )
```
